32 devices in a mesh: ep: 8 (over z, y), tp: 4 (over x, core).
Axes of the slice: x: 2, y: 2, z: 4, core: 2. Of those that a mesh axis runs over, the one named last changes fastest.
Arguments:
- query: bfloat16 [1024, 1536], P('ep', 'tp'), may hold values from -136 to 136
- latent: bfloat16 [1024, 512], P(('ep', 'tp')), may hold values from -6 to 6
- rope_key: bfloat16 [1024, 32], P(('ep', 'tp')), may hold values from -6 to 6
- latent_gain: float32 [512], replicated, may hold values from 0.1 to 1.9
- key_up: bfloat16 [512, 1024], P(None, 'tp'), may hold values from -0.25 to 0.25
- value_up: bfloat16 [512, 1024], P(None, 'tp'), may hold values from -2 to 2
- out_proj: bfloat16 [1024, 2048], replicated, may hold values from -0.1875 to 0.1875
- tokens: bfloat16 [2048, 2048], P(('ep', 'tp')), may hold values from -6 to 6
- moe_gain: float32 [2048], replicated, may hold values from 0.1 to 1.9
- routes: int32 [2048, 2], P(('ep', 'tp')), may hold values from 0 to 7, all different within a row; in each aligned block of 64 rows (0 to 63, 64 to 127, ...) at most 32 rows name the same one
- group_prob: float32 [2048], P(('ep', 'tp')), may hold values from 0.25 to 1
- expert_prob: float32 [2048, 2], P(('ep', 'tp')), may hold values from 0.02 to 1
- w_gate: bfloat16 [8, 2048, 1024], P('ep', None, 'tp'), may hold values from -0.125 to 0.125
- w_up: bfloat16 [8, 2048, 1024], P('ep', None, 'tp'), may hold values from -0.125 to 0.125
- w_down: bfloat16 [8, 1024, 2048], P('ep', 'tp'), may hold values from -0.1875 to 0.1875
Outputs:
- mixed: bfloat16 [1024, 2048], P(('ep', 'tp'))
- moe_out: bfloat16 [2048, 2048], P(('ep', 'tp'))
The draws below stay inside these ranges and needn't reach their ends.
Inputs may be any that keep to these rules, and one draw needn't show every extreme that they name: `routes`: each row names 2 different experts; within the rows of one device no expert is named more than 32 times.
All inputs are finite; a program needn't handle non-finite values.
Results may differ from the reference program's by a relative error of at most 0.025.
Values may be sent and summed in bfloat16 or wider, within the bound.
A program may use at most 128 MiB of HBM per device.

```python
import functools
import math
import jax
import jax.numpy as jnp
import numpy as np
from jax import lax

D = 2048
HEADS = 16
NOPE = 64
ROPE_DIM = 32
V_DIM = 64
LATENT = 512
EXPERT_WIDTH = 1024
TOP = 2
M_ROWS = 64
SEQ = 1024
MOE_TOKENS = 2048
EXPERTS = 8
CAP = 32
N_TP = 4


def draw_query(key, part):
    first_key = jax.random.fold_in(jax.random.fold_in(key, 11), 0)
    full_shape = (SEQ, HEADS * (NOPE + ROPE_DIM))
    values = jnp.clip(2.0 * jax.random.normal(first_key, full_shape, jnp.float32), -8.0, 8.0)
    return values.astype(jnp.bfloat16)


def block_scale(own_key, dims, cuts, smallest, top_value):
    def one(position, blocks):
        draws = jax.random.uniform(jax.random.fold_in(jax.random.fold_in(own_key, 6), position), (blocks,), jnp.float32, smallest / len(cuts), top_value / len(cuts))
        return jnp.repeat(jnp.exp(draws), dims[position] // blocks).reshape((-1,) + (1,) * (len(dims) - position - 1))

    factor_of = one(*cuts[0])
    for cut in cuts[1:]:
        factor_of = factor_of * one(*cut)
    return factor_of


def assign_block(stream_key, own, number, rows, count, top, most, slope):
    order = jax.random.permutation(stream_key, count)
    crowded, usual = portions_of(count, rows * top, most, slope, True), portions_of(count, rows * top, most, slope, False)
    places = jnp.arange(count)

    def named(lengths, turn):
        used = int((lengths > 0).sum())
        fixed = max(1, used // 4)
        shifted = fixed + (places - fixed + turn * (used - fixed)) % max(1, count - fixed)
        return jnp.zeros((count,), jnp.int32).at[order[jnp.where(places < fixed, places, shifted)]].set(jnp.asarray(lengths, jnp.int32))

    lengths = jnp.where(number % 4 == 0, named(crowded, number // 4), named(usual, number - number // 4 - 1))
    mixed = jax.random.permutation(jax.random.fold_in(own, 3), count)
    source_of, taker = mixed[0:count // 2 * 2:2], mixed[1:count // 2 * 2:2]
    room = jnp.minimum(lengths[source_of] - 1, most - lengths[taker]) // 2
    room = jnp.where((source_of == order[0]) | (taker == order[0]) | (lengths[taker] == 0), 0, jnp.maximum(room, 0))
    shifted = jax.random.randint(jax.random.fold_in(own, 4), (count // 2,), 0, 1 << 20) % (room + 1)
    lengths = lengths.at[source_of].add(-shifted).at[taker].add(shifted)
    items = jnp.searchsorted(jnp.cumsum(lengths), jnp.arange(rows * top), side="right").astype(jnp.int32)
    grid = items.reshape(top, rows).T
    grid = grid[jax.random.permutation(jax.random.fold_in(own, 1), rows)]
    turn = jax.random.randint(jax.random.fold_in(own, 2), (rows, 1), 0, top)
    return jnp.take_along_axis(grid, (jnp.arange(top)[None, :] + turn) % top, axis=1)


def portions_of(number_of, total, reach, slope, full):
    portions = [(1 << 20) // math.isqrt(standing ** slope) + 1 for standing in range(1, number_of + 1)]
    largest = reach if full else min(reach, max(-(-total // number_of), total * portions[0] // sum(portions)))
    least = 1 if total - largest >= number_of - 1 else 0
    given, rest = [largest] + [least] * (number_of - 1), total - largest - least * (number_of - 1)
    while rest > 0:
        movable = [i for i in range(1, number_of) if given[i] < largest] or [i for i in range(1, number_of) if given[i] < reach]
        pool, budget = sum([portions[i] for i in movable]), rest
        for i in movable:
            more = min(reach - given[i], max(1, budget * portions[i] // pool), rest)
            given[i] = given[i] + more
            rest = rest - more
    return np.array(given)


def centred(key, shape, spread, bound, cuts=(), kind=jnp.bfloat16):
    array = jax.random.normal(key, shape, jnp.float32) * spread
    if len(cuts) > 0:
        array = block_scale(key, shape, cuts, -0.22, 0.18) * array
    return jnp.clip(array, min=-bound, max=bound).astype(kind)


def setup_inputs(seed: int = 0) -> dict:
    key_list = jax.random.split(jax.random.key(seed), 16)
    query = draw_query(jax.random.fold_in(key_list[15], 71), 0)
    latent = centred(key_list[1], (SEQ, LATENT), 1.0, 6.0, ((0, 32),))
    rope_key = centred(key_list[2], (SEQ, ROPE_DIM), 1.0, 6.0, ((0, 32),))
    latent_gain = jnp.clip(1.0 + 0.18 * jax.random.normal(key_list[3], (LATENT,), jnp.float32), 0.1, 1.9)
    key_up = centred(key_list[4], (LATENT, HEADS * NOPE), LATENT ** -0.5, 0.25, ((1, 4),))
    value_up = centred(key_list[5], (LATENT, HEADS * V_DIM), (LATENT // 64) ** -0.5, 2.0, ((1, 4),))
    out_proj = centred(key_list[6], (HEADS * V_DIM, D), (HEADS * V_DIM) ** -0.5, 0.1875)
    tokens = centred(key_list[7], (MOE_TOKENS, D), 1.0, 6.0, ((0, 32),))
    moe_gain = jnp.clip(1.0 + 0.18 * jax.random.normal(key_list[8], (D,), jnp.float32), 0.1, 1.9)
    routes_keys = jax.random.split(jax.random.fold_in(key_list[9], 1), MOE_TOKENS // M_ROWS)
    routes_turns = jax.random.permutation(jax.random.fold_in(key_list[9], 3), MOE_TOKENS // M_ROWS)
    routes = jax.vmap(lambda own, number: assign_block(jax.random.fold_in(key_list[9], 2), own, number, M_ROWS, EXPERTS, TOP, CAP, 2))(routes_keys, routes_turns).reshape((MOE_TOKENS, TOP))
    group_prob = jnp.clip(jnp.exp(math.log(1.0) - 1.3862944 * jax.random.uniform(key_list[10], (MOE_TOKENS,), jnp.float32) ** block_scale(key_list[10], (MOE_TOKENS,), ((0, 32),), -0.2, 0.2)), 0.25, 1.0)
    expert_prob = jnp.clip(jnp.exp(math.log(1.0) - 3.912023 * jax.random.uniform(key_list[11], (MOE_TOKENS, TOP), jnp.float32) ** block_scale(key_list[11], (MOE_TOKENS, TOP), ((0, 32),), -0.2, 0.2)), 0.02, 1.0)
    w_gate = centred(key_list[12], (EXPERTS, D, EXPERT_WIDTH), D ** -0.5, 0.125, ((0, 8), (2, 4)))
    w_up = centred(key_list[13], (EXPERTS, D, EXPERT_WIDTH), D ** -0.5, 0.125, ((0, 8), (2, 4)))
    w_down = centred(key_list[14], (EXPERTS, EXPERT_WIDTH, D), EXPERT_WIDTH ** -0.5, 0.1875, ((0, 8), (1, 4)))
    return {"query": query, "latent": latent, "rope_key": rope_key, "latent_gain": latent_gain, "key_up": key_up, "value_up": value_up, "out_proj": out_proj, "tokens": tokens, "moe_gain": moe_gain, "routes": routes, "group_prob": group_prob, "expert_prob": expert_prob, "w_gate": w_gate, "w_up": w_up, "w_down": w_down}


epsilon = 1e-06
rope_base = 10000.0
masked_value = -1e+30

def rms_scale(values, gain):
    widened = values.astype(jnp.float32)
    return widened * lax.rsqrt(lax.optimization_barrier(jnp.mean(widened * widened, axis=-1, keepdims=True)) + epsilon) * gain.astype(jnp.float32)

def tables(positions, rope_width):
    half_width = rope_width // 2
    inverse = rope_base ** (-2.0 * jnp.arange(half_width, dtype=jnp.float32) / rope_width)
    angles = positions.astype(jnp.float32)[:, None] * inverse[None, :]
    return (jnp.cos(angles), jnp.sin(angles))

def rotate(values, cosine, sine):
    half_width = values.shape[-1] // 2
    lower = values[..., :half_width]
    upper = values[..., half_width:]
    return jnp.concatenate([lower * cosine - upper * sine, lower * sine + upper * cosine], axis=-1)

def head_attention(rope_prefix, query_pos, parts):
    query_head, key_head, value_head = parts
    full_keys = jnp.concatenate([key_head, rope_prefix], axis=-1)
    scores = jnp.dot(query_head, full_keys.T, preferred_element_type=jnp.float32) * (NOPE + ROPE_DIM) ** (-0.5)
    key_pos = jnp.arange(full_keys.shape[0], dtype=jnp.int32)
    allowed = key_pos[None, :] <= query_pos[:, None]
    scores = jnp.where(allowed, scores, masked_value)
    row_peak = lax.optimization_barrier(jnp.max(scores, axis=-1, keepdims=True))
    raised = jnp.where(allowed, jnp.exp(scores - row_peak), 0.0)
    totals = lax.optimization_barrier(jnp.sum(raised, axis=-1, keepdims=True))
    summed = jnp.dot(raised.astype(jnp.bfloat16), value_head, preferred_element_type=jnp.float32)
    return (summed / totals).astype(jnp.bfloat16)

def mixer_reference(query, latent, rope_key, latent_gain, key_up, value_up, out_proj):
    seq_len = latent.shape[0]
    positions = jnp.arange(seq_len, dtype=jnp.int32)
    cosine, sine = tables(positions, ROPE_DIM)
    normed = rms_scale(latent, latent_gain).astype(jnp.bfloat16)
    rotated_key = rotate(rope_key.astype(jnp.float32), cosine, sine).astype(jnp.bfloat16)
    query_heads = query.reshape(seq_len, HEADS, NOPE + ROPE_DIM)
    turned = rotate(query_heads[..., NOPE:].astype(jnp.float32), cosine[:, None, :], sine[:, None, :]).astype(jnp.bfloat16)
    rotated_query = jnp.concatenate([query_heads[..., :NOPE], turned], axis=-1)
    key_nope = jnp.dot(normed, key_up, preferred_element_type=jnp.float32).astype(jnp.bfloat16).reshape(seq_len, HEADS, NOPE)
    values = jnp.dot(normed, value_up, preferred_element_type=jnp.float32).astype(jnp.bfloat16).reshape(seq_len, HEADS, V_DIM)
    block_len = math.gcd(seq_len, 512)
    pieces = []
    for block_at in range(seq_len // block_len):
        upto = (block_at + 1) * block_len
        query_pos = positions[block_at * block_len:upto]
        parts = (rotated_query[block_at * block_len:upto].transpose(1, 0, 2), key_nope[:upto].transpose(1, 0, 2), values[:upto].transpose(1, 0, 2))
        result = lax.map(functools.partial(head_attention, rotated_key[:upto], query_pos), parts)
        pieces.append(result.transpose(1, 0, 2).reshape(block_len, HEADS * V_DIM))
    attention = jnp.concatenate(pieces, axis=0)
    return jnp.dot(attention, out_proj, preferred_element_type=jnp.float32).astype(jnp.bfloat16)

def expert_reference(tokens, moe_gain, routes, group_prob, expert_prob, w_gate, w_up, w_down):
    amount = tokens.shape[0]
    model_width = tokens.shape[1]
    expert_count = w_gate.shape[0]
    block_count = amount // M_ROWS
    normed = rms_scale(tokens, moe_gain).astype(jnp.bfloat16)
    flat_routes = routes.reshape(block_count, M_ROWS * TOP)
    onehot = (flat_routes[:, :, None] == jnp.arange(expert_count, dtype=jnp.int32)[None, None, :]).astype(jnp.int32)
    earlier = jnp.cumsum(onehot, axis=1) - onehot
    slot_index = lax.optimization_barrier(jnp.sum(earlier * onehot, axis=2))
    block_ids = jnp.arange(block_count, dtype=jnp.int32)[:, None]
    place = block_ids * CAP + slot_index
    source_row = block_ids * M_ROWS + jnp.arange(M_ROWS * TOP, dtype=jnp.int32)[None, :] // TOP
    shares = group_prob[:, None] * expert_prob / lax.optimization_barrier(jnp.sum(expert_prob, axis=1, keepdims=True))
    row_table = jnp.full((expert_count, block_count * CAP), amount, jnp.int32).at[flat_routes, place].set(source_row)
    share_table = jnp.zeros((expert_count, block_count * CAP), jnp.float32).at[flat_routes, place].set(shares.reshape(block_count, M_ROWS * TOP))
    padded = jnp.concatenate([normed, jnp.zeros((1, model_width), jnp.bfloat16)], axis=0)
    group_width = w_down.shape[1] // N_TP

    def per_expert(running, parts):
        row_ids, row_shares, gate_weight, up_weight, down_weight = parts
        rows_here = padded[row_ids]
        gate_values = jnp.dot(rows_here, gate_weight, preferred_element_type=jnp.float32)
        up_values = jnp.dot(rows_here, up_weight, preferred_element_type=jnp.float32)
        hidden = (jax.nn.silu(gate_values) * up_values).astype(jnp.bfloat16)
        summed = jnp.zeros((rows_here.shape[0], model_width), jnp.float32)
        for group_at in range(N_TP):
            lower_edge = group_at * group_width
            partial_low = jnp.dot(hidden[:, lower_edge:lower_edge + group_width], down_weight[lower_edge:lower_edge + group_width], preferred_element_type=jnp.float32).astype(jnp.bfloat16)
            partial_low = lax.optimization_barrier(partial_low)
            summed = summed + partial_low.astype(jnp.float32)
        expert_out = summed.astype(jnp.bfloat16)
        expert_out = lax.optimization_barrier(expert_out)
        running = running.at[row_ids].add(row_shares[:, None] * expert_out.astype(jnp.float32))
        return (running, None)
    running, _ = lax.scan(per_expert, jnp.zeros((amount + 1, model_width), jnp.float32), (row_table, share_table, w_gate, w_up, w_down))
    return running[:amount].astype(jnp.bfloat16)

def reference(query, latent, rope_key, latent_gain, key_up, value_up, out_proj, tokens, moe_gain, routes, group_prob, expert_prob, w_gate, w_up, w_down):
    mixed = mixer_reference(query, latent, rope_key, latent_gain, key_up, value_up, out_proj)
    moe_out = expert_reference(tokens, moe_gain, routes, group_prob, expert_prob, w_gate, w_up, w_down)
    return (mixed, moe_out)
```

```python
import functools
import math

import jax
import jax.numpy as jnp
from jax import lax
from jax.experimental import pallas as pl
from jax.experimental.pallas import tpu as pltpu
from jax.sharding import PartitionSpec as P

NOPE = 64
ROPE_DIM = 32
V_DIM = 64


epsilon = 1e-06
rope_base = 10000.0
masked_value = -1e30


def rms_scale(values, gain):
    widened = values.astype(jnp.float32)
    return widened * lax.rsqrt(jnp.mean(widened * widened, axis=-1, keepdims=True) + epsilon) * gain


def tables(positions, rope_width):
    half_width = rope_width // 2
    inverse = rope_base ** (-2.0 * jnp.arange(half_width, dtype=jnp.float32) / rope_width)
    angles = positions.astype(jnp.float32)[:, None] * inverse[None, :]
    return (jnp.cos(angles), jnp.sin(angles))


def rotate(values, cosine, sine):
    half_width = values.shape[-1] // 2
    lower = values[..., :half_width]
    upper = values[..., half_width:]
    return jnp.concatenate([lower * cosine - upper * sine, lower * sine + upper * cosine], axis=-1)


def keep_state(state_in):
    return state_in


def attend_block(running, query_rot, query_pos, key_part, value_part, rope_part):
    amount = key_part.shape[0]
    span_rows = math.gcd(amount, 1024)
    head_count = query_rot.shape[1]
    scale_factor = query_rot.shape[2] ** (-0.5)
    last_query = query_pos[-1]

    def update(state, block_at):
        row_begin = block_at * span_rows
        keys_here = lax.dynamic_slice_in_dim(key_part, row_begin, span_rows, 0).reshape(
            span_rows, head_count, -1
        )
        values_here = lax.dynamic_slice_in_dim(value_part, row_begin, span_rows, 0).reshape(
            span_rows, head_count, -1
        )
        rope_here = lax.dynamic_slice_in_dim(rope_part, row_begin, span_rows, 0)
        key_pos = row_begin + jnp.arange(span_rows, dtype=jnp.int32)

        def advance(state_in):
            top_old, totals, weighted = state_in
            shared = jnp.broadcast_to(
                rope_here[:, None, :], (span_rows, head_count, rope_here.shape[1])
            )
            full_keys = jnp.concatenate([keys_here, shared], axis=-1)
            scores = (
                jnp.einsum("qhd,khd->hqk", query_rot, full_keys, preferred_element_type=jnp.float32)
                * scale_factor
            )
            allowed = key_pos[None, :] <= query_pos[:, None]
            scores = jnp.where(allowed[None], scores, masked_value)
            top_new = jnp.maximum(top_old, jnp.max(scores, axis=-1))
            raised = jnp.where(allowed[None], jnp.exp(scores - top_new[..., None]), 0.0)
            factor = jnp.exp(top_old - top_new)
            totals = totals * factor + jnp.sum(raised, axis=-1)
            weighted = weighted * factor[..., None] + jnp.einsum(
                "hqk,khd->hqd",
                raised.astype(jnp.bfloat16),
                values_here,
                preferred_element_type=jnp.float32,
            )
            return (top_new, totals, weighted)

        return (lax.cond(key_pos[0] <= last_query, advance, keep_state, state), None)

    running, _ = lax.scan(update, running, jnp.arange(amount // span_rows))
    return running


def mixer_half(query, latent, rope_key, latent_gain, key_up, value_up, out_proj):
    query_rows = query.shape[0]
    own_rows = latent.shape[0]
    query_start = lax.axis_index("ep") * query_rows
    key_start = query_start + lax.axis_index("tp") * own_rows
    head_count = query.shape[1] // (NOPE + ROPE_DIM)
    normed = rms_scale(latent, latent_gain).astype(jnp.bfloat16)
    key_cos, key_sin = tables(key_start + jnp.arange(own_rows, dtype=jnp.int32), ROPE_DIM)
    rotated_key = rotate(rope_key.astype(jnp.float32), key_cos, key_sin).astype(jnp.bfloat16)
    query_pos = query_start + jnp.arange(query_rows, dtype=jnp.int32)
    query_cos, query_sin = tables(query_pos, ROPE_DIM)
    query_heads = query.reshape(query_rows, head_count, NOPE + ROPE_DIM)
    turned = rotate(
        query_heads[..., NOPE:].astype(jnp.float32), query_cos[:, None, :], query_sin[:, None, :]
    ).astype(jnp.bfloat16)
    query_rot = jnp.concatenate([query_heads[..., :NOPE], turned], axis=-1)
    last_query = query_start + query_rows - 1
    initial = (
        jnp.full((head_count, query_rows), masked_value, jnp.float32),
        jnp.zeros((head_count, query_rows), jnp.float32),
        jnp.zeros((head_count, query_rows, V_DIM), jnp.float32),
    )
    shard_rows = (
        lax.all_gather(normed, ("ep", "tp"), axis=0, tiled=True),
        lax.all_gather(rotated_key, ("ep", "tp"), axis=0, tiled=True),
    )

    def compute(state_in):
        key_part = jnp.dot(shard_rows[0], key_up, preferred_element_type=jnp.float32).astype(
            jnp.bfloat16
        )
        value_part = jnp.dot(shard_rows[0], value_up, preferred_element_type=jnp.float32).astype(
            jnp.bfloat16
        )
        return attend_block(state_in, query_rot, query_pos, key_part, value_part, shard_rows[1])

    running = lax.cond(jnp.int32(0) <= last_query, compute, keep_state, initial)
    totals = running[1]
    weighted = running[2]
    attention = (
        (weighted / totals[..., None])
        .transpose(1, 0, 2)
        .reshape(query_rows, head_count * V_DIM)
        .astype(jnp.bfloat16)
    )
    own_attention = lax.all_to_all(attention, "tp", split_axis=0, concat_axis=1, tiled=True)
    return jnp.dot(own_attention, out_proj, preferred_element_type=jnp.float32).astype(jnp.bfloat16)


def expert_half(tokens, moe_gain, routes, group_prob, expert_prob, w_gate, w_up, w_down):
    row_count, model_width = tokens.shape
    top_count = routes.shape[1]
    expert_count = lax.axis_size("ep")
    capacity = 2 * top_count * row_count // expert_count
    normed = rms_scale(tokens, moe_gain).astype(jnp.bfloat16)
    flat_routes = routes.reshape(-1)
    onehot = (flat_routes[:, None] == jnp.arange(expert_count, dtype=jnp.int32)[None, :]).astype(
        jnp.int32
    )
    earlier = jnp.cumsum(onehot, axis=0) - onehot
    slot_index = jnp.sum(earlier * onehot, axis=1)
    target = flat_routes * capacity + slot_index
    owner = target[None, :] == jnp.arange(expert_count * capacity, dtype=jnp.int32)[:, None]
    dispatch_table = jnp.any(
        owner.reshape(expert_count * capacity, row_count, top_count), axis=2
    ).astype(jnp.bfloat16)
    outgoing = jnp.dot(dispatch_table, normed, preferred_element_type=jnp.float32).astype(
        jnp.bfloat16
    )
    outgoing = outgoing.reshape(expert_count, capacity, model_width)
    arrived = lax.all_to_all(outgoing, "ep", split_axis=0, concat_axis=0, tiled=True)
    sources, slots, _ = arrived.shape
    flat_rows = arrived.reshape(sources * slots, model_width)
    shard_rows = lax.all_gather(flat_rows, "tp", axis=0, tiled=True)
    gate_values = jnp.dot(shard_rows, w_gate[0], preferred_element_type=jnp.float32)
    up_values = jnp.dot(shard_rows, w_up[0], preferred_element_type=jnp.float32)
    hidden = (jax.nn.silu(gate_values) * up_values).astype(jnp.bfloat16)

    def lower(offset, amount):
        return jnp.dot(hidden, w_down[0], preferred_element_type=jnp.float32)

    summed = lax.psum_scatter(
        lower(jnp.int32(0), sources * slots * lax.axis_size("tp")).astype(jnp.bfloat16),
        "tp",
        scatter_dimension=0,
        tiled=True,
    )
    result = summed.reshape(sources, slots, model_width)
    returned = lax.all_to_all(result, "ep", split_axis=0, concat_axis=0, tiled=True)
    returned_flat = returned.reshape(expert_count * capacity, model_width)
    picked = returned_flat[target].reshape(row_count, top_count, model_width).astype(jnp.float32)
    shares = group_prob[:, None] * expert_prob / jnp.sum(expert_prob, axis=1, keepdims=True)
    return jnp.sum(shares[:, :, None] * picked, axis=1).astype(jnp.bfloat16)


def body(
    query,
    latent,
    rope_key,
    latent_gain,
    key_up,
    value_up,
    out_proj,
    tokens,
    moe_gain,
    routes,
    group_prob,
    expert_prob,
    w_gate,
    w_up,
    w_down,
):
    mixed = mixer_half(query, latent, rope_key, latent_gain, key_up, value_up, out_proj)
    moe_out = expert_half(tokens, moe_gain, routes, group_prob, expert_prob, w_gate, w_up, w_down)
    return (mixed, moe_out)


def both_halves(
    heads,
    rope_width,
    outgoing,
    lat_own,
    query_big,
    key_up,
    value_up,
    out_proj_hbm,
    gate_hbm,
    up_hbm,
    down_hbm,
    mixed,
    returned,
    arrived,
    lat_all,
    partial,
    from_pair,
    pair_sum,
    from_far,
    result,
    keys,
    heads_own,
    heads_all,
    out_proj,
    gate,
    up,
    down,
    load_sem,
    send_sem,
    recv_sem,
    head_send,
    head_recv,
):
    experts, capacity, width = outgoing.shape
    n_tp = lat_all.shape[1]
    me = lax.axis_index("ep")
    tp = lax.axis_index("tp")
    mate = tp + 1 - 2 * (tp % 2)
    far = (tp + 2) % n_tp
    cross = (mate + 2) % n_tp

    loads = [
        pltpu.make_async_copy(gate_hbm, gate, load_sem.at[0]),
        pltpu.make_async_copy(up_hbm, up, load_sem.at[1]),
        pltpu.make_async_copy(down_hbm, down, load_sem.at[2]),
        pltpu.make_async_copy(out_proj_hbm, out_proj, load_sem.at[3]),
        pltpu.make_async_copy(outgoing.at[me], arrived.at[me, tp], load_sem.at[4]),
        pltpu.make_async_copy(lat_own, lat_all.at[me, tp], load_sem.at[5]),
    ]
    for load in loads:
        load.start()

    def remote(src, dst, kind, step, device):
        return pltpu.make_async_remote_copy(
            src_ref=src,
            dst_ref=dst,
            send_sem=send_sem.at[kind, step],
            recv_sem=recv_sem.at[kind, step],
            device_id=device,
            device_id_type=pl.DeviceIdType.MESH,
        )

    barrier = pltpu.get_barrier_semaphore()

    def greet(step, carry):
        pl.semaphore_signal(
            barrier,
            inc=1,
            device_id={"ep": (me + step) % experts},
            device_id_type=pl.DeviceIdType.MESH,
        )
        return carry

    lax.fori_loop(1, experts, greet, 0)
    for peer in (mate, far, cross):
        pl.semaphore_signal(
            barrier, inc=1, device_id={"tp": peer}, device_id_type=pl.DeviceIdType.MESH
        )
    pl.semaphore_wait(barrier, experts + 2)

    def ep_rows(step, slot):
        target = (me + step) % experts
        return remote(outgoing.at[target], arrived.at[slot, tp], 0, step, {"ep": target})

    def ep_lat(step, slot):
        target = (me + step) % experts
        return remote(lat_own, lat_all.at[slot, tp], 1, step, {"ep": target})

    def hop_rows(kind, step, block, peer):
        source = (me + experts - step) % experts
        place = arrived.at[source, block]
        return remote(place, place, kind, step, {"tp": peer})

    def hop_lat(kind, step, block, peer):
        source = (me + experts - step) % experts
        place = lat_all.at[source, block]
        return remote(place, place, kind, step, {"tp": peer})

    def to_mate(kind, step, block, part):
        source = (me + experts - step) % experts
        return remote(
            partial.at[source, block], from_pair.at[source, part], kind, step, {"tp": mate}
        )

    def to_far(step):
        source = (me + experts - step) % experts
        return remote(pair_sum.at[source], from_far.at[source], 10, step, {"tp": far})

    def back(step, slot):
        source = (me + experts - step) % experts
        return remote(result.at[source], returned.at[slot], 11, step, {"ep": source})

    def send_all(step, carry):
        ep_lat(step, me).start()
        return carry

    lax.fori_loop(1, experts, send_all, 0)

    def send_rows(step, carry):
        ep_rows(step, me).start()
        return carry

    lax.fori_loop(1, experts, send_rows, 0)
    for load in loads[4:]:
        load.wait()

    def forward(step):
        source = (me + experts - step) % experts

        @pl.when(step > 0)
        def _():
            ep_lat(step, source).wait_recv()
            ep_rows(step, source).wait_recv()

        hop_lat(5, step, tp, far).start()
        hop_rows(4, step, tp, far).start()
        hop_lat(3, step, tp, mate).start()
        hop_rows(2, step, tp, mate).start()

    def relay(step):
        hop_lat(5, step, far, far).wait_recv()
        hop_rows(4, step, far, far).wait_recv()
        hop_lat(7, step, far, mate).start()
        hop_rows(6, step, far, mate).start()

    def compute(step):
        source = (me + experts - step) % experts
        hop_lat(3, step, mate, mate).wait_recv()
        hop_rows(2, step, mate, mate).wait_recv()
        hop_lat(7, step, cross, mate).wait_recv()
        hop_rows(6, step, cross, mate).wait_recv()

        @pl.when(step == 0)
        def _():
            for load in loads[:3]:
                load.wait()

        rows = arrived[source].reshape(n_tp * capacity, width)
        gate_values = jnp.dot(rows, gate[...], preferred_element_type=jnp.float32)
        up_values = jnp.dot(rows, up[...], preferred_element_type=jnp.float32)
        hidden = (gate_values / (1.0 + jnp.exp(-gate_values)) * up_values).astype(jnp.bfloat16)
        product = jnp.dot(hidden, down[...], preferred_element_type=jnp.float32)
        partial[source] = product.astype(jnp.bfloat16).reshape(n_tp, capacity, width)
        to_mate(9, step, cross, 1).start()
        to_mate(8, step, mate, 0).start()

    def reduce_pair(step):
        source = (me + experts - step) % experts
        to_mate(9, step, cross, 1).wait_recv()
        pair_sum[source] = (
            partial[source, far].astype(jnp.float32) + from_pair[source, 1].astype(jnp.float32)
        ).astype(jnp.bfloat16)
        to_far(step).start()

    def reduce_far(step):
        source = (me + experts - step) % experts
        to_mate(8, step, mate, 0).wait_recv()
        to_far(step).wait_recv()
        result[source] = (
            partial[source, tp].astype(jnp.float32)
            + from_pair[source, 0].astype(jnp.float32)
            + from_far[source].astype(jnp.float32)
        ).astype(jnp.bfloat16)

        @pl.when(step > 0)
        def _():
            back(step, me).start()

        @pl.when(step == 0)
        def _():
            returned[me] = result[me]

    def attend():
        rows = query_big.shape[1]
        latent_width = key_up.shape[0]
        nope_width = key_up.shape[1]
        value_width = value_up.shape[1] // heads
        packed = lat_all[...].reshape(-1, lat_all.shape[-1])
        normed = packed[:, :latent_width]
        seq = packed.shape[0]
        keys[:, :nope_width] = jnp.dot(
            normed, key_up[...], preferred_element_type=jnp.float32
        ).astype(jnp.bfloat16)
        keys[:, nope_width:] = packed[:, latent_width:]
        values = jnp.dot(normed, value_up[...], preferred_element_type=jnp.float32).astype(
            jnp.bfloat16
        )
        query_pos = me * rows + lax.broadcasted_iota(jnp.int32, (rows, seq), 0)
        allowed = lax.broadcasted_iota(jnp.int32, (rows, seq), 1) <= query_pos
        lane = lax.broadcasted_iota(jnp.int32, (rows, heads * value_width), 1)
        scale = (nope_width // heads + rope_width) ** (-0.5)
        gathered = jnp.zeros((rows, heads * value_width), jnp.float32)
        for head in range(heads):
            scores = (
                lax.dot_general(
                    query_big[head],
                    keys[...],
                    (((1,), (1,)), ((), ())),
                    preferred_element_type=jnp.float32,
                )
                * scale
            )
            scores = jnp.where(allowed, scores, masked_value)
            raised = jnp.exp(scores - jnp.max(scores, axis=1, keepdims=True))
            totals = jnp.sum(raised, axis=1, keepdims=True)
            weighted = jnp.dot(
                raised.astype(jnp.bfloat16), values, preferred_element_type=jnp.float32
            )
            inside = (lane >= head * value_width) & (lane < (head + 1) * value_width)
            gathered = jnp.where(inside, weighted / totals, gathered)
        heads_own[...] = gathered.astype(jnp.bfloat16).reshape(heads_own.shape)

    def head_copy(number, peer, slot):
        return pltpu.make_async_remote_copy(
            src_ref=heads_own.at[peer],
            dst_ref=heads_all.at[slot],
            send_sem=head_send.at[number],
            recv_sem=head_recv.at[number],
            device_id={"tp": peer},
            device_id_type=pl.DeviceIdType.MESH,
        )

    def stage(turn, carry):
        @pl.when(turn < experts)
        def _():
            forward(turn)

        @pl.when((turn >= 1) & (turn < experts + 1))
        def _():
            relay(turn - 1)

        @pl.when((turn >= 2) & (turn < experts + 2))
        def _():
            compute(turn - 2)

        @pl.when((turn >= 3) & (turn < experts + 3))
        def _():
            reduce_pair(turn - 3)

        @pl.when(turn >= 4)
        def _():
            reduce_far(turn - 4)

        return carry

    lax.fori_loop(0, experts + 4, stage, 0)

    attend()
    peers = (mate, far, cross)
    for number, peer in enumerate(peers):
        head_copy(number, peer, tp).start()
    heads_all[tp] = heads_own[tp]
    loads[3].wait()
    for number, peer in enumerate(peers):
        head_copy(number, peer, peer).wait_recv()
    depth = heads_all.shape[2]
    total = jnp.zeros(mixed.shape, jnp.float32)
    for part in range(n_tp):
        total = total + jnp.dot(
            heads_all[part],
            out_proj[part * depth : (part + 1) * depth, :],
            preferred_element_type=jnp.float32,
        )
    mixed[...] = total.astype(mixed.dtype)

    def finish(step, carry):
        ep_lat(step, me).wait_send()
        ep_rows(step, me).wait_send()
        back(step, me).wait_send()
        back(step, (me + step) % experts).wait_recv()
        return carry

    lax.fori_loop(1, experts, finish, 0)

    def finish_tp(step, carry):
        hop_lat(5, step, tp, far).wait_send()
        hop_rows(4, step, tp, far).wait_send()
        hop_lat(3, step, tp, mate).wait_send()
        hop_rows(2, step, tp, mate).wait_send()
        hop_lat(7, step, far, mate).wait_send()
        hop_rows(6, step, far, mate).wait_send()
        to_mate(9, step, cross, 1).wait_send()
        to_mate(8, step, mate, 0).wait_send()
        to_far(step).wait_send()
        return carry

    lax.fori_loop(0, experts, finish_tp, 0)
    for number, peer in enumerate(peers):
        head_copy(number, peer, tp).wait_send()


def padded(amount):
    return -(-amount // 128) * 128


def fused_body(
    query,
    latent,
    rope_key,
    latent_gain,
    key_up,
    value_up,
    out_proj,
    tokens,
    moe_gain,
    routes,
    group_prob,
    expert_prob,
    w_gate,
    w_up,
    w_down,
):
    n_ep = lax.axis_size("ep")
    n_tp = lax.axis_size("tp")
    query_rows = query.shape[0]
    own_rows, latent_width = latent.shape
    query_start = lax.axis_index("ep") * query_rows
    key_start = query_start + lax.axis_index("tp") * own_rows
    heads = query.shape[1] // (NOPE + ROPE_DIM)
    normed_latent = rms_scale(latent, latent_gain).astype(jnp.bfloat16)
    key_cos, key_sin = tables(key_start + jnp.arange(own_rows, dtype=jnp.int32), ROPE_DIM)
    rotated_key = rotate(rope_key.astype(jnp.float32), key_cos, key_sin).astype(jnp.bfloat16)
    rope_room = padded(ROPE_DIM)
    gap = rope_room - ROPE_DIM
    lat_own = jnp.concatenate([normed_latent, jnp.pad(rotated_key, ((0, 0), (0, gap)))], axis=1)
    query_cos, query_sin = tables(query_start + jnp.arange(query_rows, dtype=jnp.int32), ROPE_DIM)
    query_heads = query.reshape(query_rows, heads, NOPE + ROPE_DIM).transpose(1, 0, 2)
    turned = rotate(
        query_heads[..., NOPE:].astype(jnp.float32), query_cos[None], query_sin[None]
    ).astype(jnp.bfloat16)
    own_head = jnp.eye(heads, dtype=jnp.bool_)[:, None, :, None]
    spread = jnp.where(own_head, query_heads[:, :, None, :NOPE], jnp.bfloat16(0)).reshape(
        heads, query_rows, heads * NOPE
    )
    query_big = jnp.concatenate(
        [spread, jnp.pad(turned, ((0, 0), (0, 0), (0, gap)))], axis=-1
    )

    row_count, width = tokens.shape
    top_count = routes.shape[1]
    capacity = 2 * top_count * row_count // n_ep
    normed = rms_scale(tokens, moe_gain).astype(jnp.bfloat16)
    flat_routes = routes.reshape(-1)
    onehot = (flat_routes[:, None] == jnp.arange(n_ep, dtype=jnp.int32)[None, :]).astype(jnp.int32)
    earlier = jnp.cumsum(onehot, axis=0) - onehot
    slot_index = jnp.sum(earlier * onehot, axis=1)
    target = flat_routes * capacity + slot_index
    owner = target[None, :] == jnp.arange(n_ep * capacity, dtype=jnp.int32)[:, None]
    dispatch_table = jnp.any(owner.reshape(n_ep * capacity, row_count, top_count), axis=2).astype(
        jnp.bfloat16
    )
    outgoing = jnp.dot(dispatch_table, normed, preferred_element_type=jnp.float32).astype(
        jnp.bfloat16
    )
    outgoing = outgoing.reshape(n_ep, capacity, width)

    bf16 = jnp.bfloat16
    lat_width = latent_width + rope_room
    vmem = pl.BlockSpec(memory_space=pltpu.VMEM)
    anywhere = pl.BlockSpec(memory_space=pl.ANY)
    mixed, returned = pl.pallas_call(
        functools.partial(both_halves, heads, ROPE_DIM),
        out_shape=(
            jax.ShapeDtypeStruct((own_rows, out_proj.shape[1]), bf16),
            jax.ShapeDtypeStruct((n_ep, capacity, width), bf16),
        ),
        in_specs=[vmem] * 5 + [anywhere] * 4,
        out_specs=(vmem, vmem),
        scratch_shapes=[
            pltpu.VMEM((n_ep, n_tp, capacity, width), bf16),
            pltpu.VMEM((n_ep, n_tp, own_rows, lat_width), bf16),
            pltpu.VMEM((n_ep, n_tp, capacity, width), bf16),
            pltpu.VMEM((n_ep, 2, capacity, width), bf16),
            pltpu.VMEM((n_ep, capacity, width), bf16),
            pltpu.VMEM((n_ep, capacity, width), bf16),
            pltpu.VMEM((n_ep, capacity, width), bf16),
            pltpu.VMEM((n_ep * n_tp * own_rows, key_up.shape[1] + rope_room), bf16),
            pltpu.VMEM((n_tp, own_rows, value_up.shape[1]), bf16),
            pltpu.VMEM((n_tp, own_rows, value_up.shape[1]), bf16),
            pltpu.VMEM(out_proj.shape, bf16),
            pltpu.VMEM(w_gate.shape[1:], bf16),
            pltpu.VMEM(w_up.shape[1:], bf16),
            pltpu.VMEM(w_down.shape[1:], bf16),
            pltpu.SemaphoreType.DMA((6,)),
            pltpu.SemaphoreType.DMA((12, n_ep)),
            pltpu.SemaphoreType.DMA((12, n_ep)),
            pltpu.SemaphoreType.DMA((3,)),
            pltpu.SemaphoreType.DMA((3,)),
        ],
        compiler_params=pltpu.CompilerParams(
            collective_id=0, has_side_effects=True, vmem_limit_bytes=56 * 1024 * 1024
        ),
        name="both_halves",
    )(
        outgoing,
        lat_own,
        query_big,
        key_up,
        value_up,
        out_proj,
        w_gate[0],
        w_up[0],
        w_down[0],
    )
    flat = returned.reshape(n_ep * capacity, width)
    picked = flat[target].reshape(row_count, top_count, width).astype(jnp.float32)
    shares = group_prob[:, None] * expert_prob / jnp.sum(expert_prob, axis=1, keepdims=True)
    moe_out = jnp.sum(shares[:, :, None] * picked, axis=1).astype(bf16)
    return (mixed, moe_out)


def fits_kernel(mesh, *arrays):
    n_ep, n_tp = mesh.shape["ep"], mesh.shape["tp"]
    tokens, routes, latent = arrays[7], arrays[9], arrays[1]
    capacity = 2 * routes.shape[1] * tokens.shape[0] // (n_ep * n_tp) // n_ep
    own_rows = latent.shape[0] // (n_ep * n_tp)
    packed = latent.shape[0] <= 2048
    return n_tp == 4 and capacity % 16 == 0 and own_rows % 16 == 0 and packed


def mapped(mesh, chosen):
    return jax.shard_map(
        chosen,
        mesh=mesh,
        in_specs=(
            P("ep", "tp"),
            P(("ep", "tp"), None),
            P(("ep", "tp"), None),
            P(),
            P(None, "tp"),
            P(None, "tp"),
            P(),
            P(("ep", "tp"), None),
            P(),
            P(("ep", "tp"), None),
            P(("ep", "tp")),
            P(("ep", "tp"), None),
            P("ep", None, "tp"),
            P("ep", None, "tp"),
            P("ep", "tp", None),
        ),
        out_specs=(P(("ep", "tp"), None), P(("ep", "tp"), None)),
        check_vma=False,
    )


def solution(mesh):
    def whole(*arrays):
        chosen = fused_body if fits_kernel(mesh, *arrays) else body
        return mapped(mesh, chosen)(*arrays)

    return whole
```

```python
import functools
import math

import jax
import jax.numpy as jnp
from jax import lax
from jax.experimental import pallas as pl
from jax.experimental.pallas import tpu as pltpu
from jax.sharding import PartitionSpec as P

NOPE = 64
ROPE_DIM = 32
V_DIM = 64


epsilon = 1e-06
rope_base = 10000.0
masked_value = -1e30


def rms_scale(values, gain):
    widened = values.astype(jnp.float32)
    return widened * lax.rsqrt(jnp.mean(widened * widened, axis=-1, keepdims=True) + epsilon) * gain


def tables(positions, rope_width):
    half_width = rope_width // 2
    inverse = rope_base ** (-2.0 * jnp.arange(half_width, dtype=jnp.float32) / rope_width)
    angles = positions.astype(jnp.float32)[:, None] * inverse[None, :]
    return (jnp.cos(angles), jnp.sin(angles))


def rotate(values, cosine, sine):
    half_width = values.shape[-1] // 2
    lower = values[..., :half_width]
    upper = values[..., half_width:]
    return jnp.concatenate([lower * cosine - upper * sine, lower * sine + upper * cosine], axis=-1)


def keep_state(state_in):
    return state_in


def attend_block(running, query_rot, query_pos, key_part, value_part, rope_part):
    amount = key_part.shape[0]
    span_rows = math.gcd(amount, 1024)
    head_count = query_rot.shape[1]
    scale_factor = query_rot.shape[2] ** (-0.5)
    last_query = query_pos[-1]

    def update(state, block_at):
        row_begin = block_at * span_rows
        keys_here = lax.dynamic_slice_in_dim(key_part, row_begin, span_rows, 0).reshape(
            span_rows, head_count, -1
        )
        values_here = lax.dynamic_slice_in_dim(value_part, row_begin, span_rows, 0).reshape(
            span_rows, head_count, -1
        )
        rope_here = lax.dynamic_slice_in_dim(rope_part, row_begin, span_rows, 0)
        key_pos = row_begin + jnp.arange(span_rows, dtype=jnp.int32)

        def advance(state_in):
            top_old, totals, weighted = state_in
            shared = jnp.broadcast_to(
                rope_here[:, None, :], (span_rows, head_count, rope_here.shape[1])
            )
            full_keys = jnp.concatenate([keys_here, shared], axis=-1)
            scores = (
                jnp.einsum("qhd,khd->hqk", query_rot, full_keys, preferred_element_type=jnp.float32)
                * scale_factor
            )
            allowed = key_pos[None, :] <= query_pos[:, None]
            scores = jnp.where(allowed[None], scores, masked_value)
            top_new = jnp.maximum(top_old, jnp.max(scores, axis=-1))
            raised = jnp.where(allowed[None], jnp.exp(scores - top_new[..., None]), 0.0)
            factor = jnp.exp(top_old - top_new)
            totals = totals * factor + jnp.sum(raised, axis=-1)
            weighted = weighted * factor[..., None] + jnp.einsum(
                "hqk,khd->hqd",
                raised.astype(jnp.bfloat16),
                values_here,
                preferred_element_type=jnp.float32,
            )
            return (top_new, totals, weighted)

        return (lax.cond(key_pos[0] <= last_query, advance, keep_state, state), None)

    running, _ = lax.scan(update, running, jnp.arange(amount // span_rows))
    return running


def mixer_half(query, latent, rope_key, latent_gain, key_up, value_up, out_proj):
    query_rows = query.shape[0]
    own_rows = latent.shape[0]
    query_start = lax.axis_index("ep") * query_rows
    key_start = query_start + lax.axis_index("tp") * own_rows
    head_count = query.shape[1] // (NOPE + ROPE_DIM)
    normed = rms_scale(latent, latent_gain).astype(jnp.bfloat16)
    key_cos, key_sin = tables(key_start + jnp.arange(own_rows, dtype=jnp.int32), ROPE_DIM)
    rotated_key = rotate(rope_key.astype(jnp.float32), key_cos, key_sin).astype(jnp.bfloat16)
    query_pos = query_start + jnp.arange(query_rows, dtype=jnp.int32)
    query_cos, query_sin = tables(query_pos, ROPE_DIM)
    query_heads = query.reshape(query_rows, head_count, NOPE + ROPE_DIM)
    turned = rotate(
        query_heads[..., NOPE:].astype(jnp.float32), query_cos[:, None, :], query_sin[:, None, :]
    ).astype(jnp.bfloat16)
    query_rot = jnp.concatenate([query_heads[..., :NOPE], turned], axis=-1)
    last_query = query_start + query_rows - 1
    initial = (
        jnp.full((head_count, query_rows), masked_value, jnp.float32),
        jnp.zeros((head_count, query_rows), jnp.float32),
        jnp.zeros((head_count, query_rows, V_DIM), jnp.float32),
    )
    shard_rows = (
        lax.all_gather(normed, ("ep", "tp"), axis=0, tiled=True),
        lax.all_gather(rotated_key, ("ep", "tp"), axis=0, tiled=True),
    )

    def compute(state_in):
        key_part = jnp.dot(shard_rows[0], key_up, preferred_element_type=jnp.float32).astype(
            jnp.bfloat16
        )
        value_part = jnp.dot(shard_rows[0], value_up, preferred_element_type=jnp.float32).astype(
            jnp.bfloat16
        )
        return attend_block(state_in, query_rot, query_pos, key_part, value_part, shard_rows[1])

    running = lax.cond(jnp.int32(0) <= last_query, compute, keep_state, initial)
    totals = running[1]
    weighted = running[2]
    attention = (
        (weighted / totals[..., None])
        .transpose(1, 0, 2)
        .reshape(query_rows, head_count * V_DIM)
        .astype(jnp.bfloat16)
    )
    own_attention = lax.all_to_all(attention, "tp", split_axis=0, concat_axis=1, tiled=True)
    return jnp.dot(own_attention, out_proj, preferred_element_type=jnp.float32).astype(jnp.bfloat16)


def expert_half(tokens, moe_gain, routes, group_prob, expert_prob, w_gate, w_up, w_down):
    row_count, model_width = tokens.shape
    top_count = routes.shape[1]
    expert_count = lax.axis_size("ep")
    capacity = 2 * top_count * row_count // expert_count
    normed = rms_scale(tokens, moe_gain).astype(jnp.bfloat16)
    flat_routes = routes.reshape(-1)
    onehot = (flat_routes[:, None] == jnp.arange(expert_count, dtype=jnp.int32)[None, :]).astype(
        jnp.int32
    )
    earlier = jnp.cumsum(onehot, axis=0) - onehot
    slot_index = jnp.sum(earlier * onehot, axis=1)
    target = flat_routes * capacity + slot_index
    owner = target[None, :] == jnp.arange(expert_count * capacity, dtype=jnp.int32)[:, None]
    dispatch_table = jnp.any(
        owner.reshape(expert_count * capacity, row_count, top_count), axis=2
    ).astype(jnp.bfloat16)
    outgoing = jnp.dot(dispatch_table, normed, preferred_element_type=jnp.float32).astype(
        jnp.bfloat16
    )
    outgoing = outgoing.reshape(expert_count, capacity, model_width)
    arrived = lax.all_to_all(outgoing, "ep", split_axis=0, concat_axis=0, tiled=True)
    sources, slots, _ = arrived.shape
    flat_rows = arrived.reshape(sources * slots, model_width)
    shard_rows = lax.all_gather(flat_rows, "tp", axis=0, tiled=True)
    gate_values = jnp.dot(shard_rows, w_gate[0], preferred_element_type=jnp.float32)
    up_values = jnp.dot(shard_rows, w_up[0], preferred_element_type=jnp.float32)
    hidden = (jax.nn.silu(gate_values) * up_values).astype(jnp.bfloat16)

    def lower(offset, amount):
        return jnp.dot(hidden, w_down[0], preferred_element_type=jnp.float32)

    summed = lax.psum_scatter(
        lower(jnp.int32(0), sources * slots * lax.axis_size("tp")).astype(jnp.bfloat16),
        "tp",
        scatter_dimension=0,
        tiled=True,
    )
    result = summed.reshape(sources, slots, model_width)
    returned = lax.all_to_all(result, "ep", split_axis=0, concat_axis=0, tiled=True)
    returned_flat = returned.reshape(expert_count * capacity, model_width)
    picked = returned_flat[target].reshape(row_count, top_count, model_width).astype(jnp.float32)
    shares = group_prob[:, None] * expert_prob / jnp.sum(expert_prob, axis=1, keepdims=True)
    return jnp.sum(shares[:, :, None] * picked, axis=1).astype(jnp.bfloat16)


def body(
    query,
    latent,
    rope_key,
    latent_gain,
    key_up,
    value_up,
    out_proj,
    tokens,
    moe_gain,
    routes,
    group_prob,
    expert_prob,
    w_gate,
    w_up,
    w_down,
):
    mixed = mixer_half(query, latent, rope_key, latent_gain, key_up, value_up, out_proj)
    moe_out = expert_half(tokens, moe_gain, routes, group_prob, expert_prob, w_gate, w_up, w_down)
    return (mixed, moe_out)


def both_halves(
    heads,
    rope_width,
    outgoing,
    lat_own,
    query_big,
    key_up,
    value_up,
    out_proj_hbm,
    gate_hbm,
    up_hbm,
    down_hbm,
    slots,
    shares,
    mixed,
    moe_out,
    returned,
    relay_in,
    relay_back,
    arrived,
    lat_all,
    partial,
    from_pair,
    pair_sum,
    from_far,
    result,
    keys,
    heads_own,
    heads_all,
    out_proj,
    gate,
    up,
    down,
    load_sem,
    send_sem,
    recv_sem,
    head_send,
    head_recv,
):
    experts, capacity, width = outgoing.shape
    n_tp = lat_all.shape[2]
    depth_z = experts // 2
    middle = depth_z + 1 if depth_z == 4 else experts
    me = lax.axis_index("ep")
    tp = lax.axis_index("tp")
    me_z = me // 2
    me_y = me % 2
    mate = tp + 1 - 2 * (tp % 2)
    far = (tp + 2) % n_tp
    cross = (mate + 2) % n_tp

    loads = [
        pltpu.make_async_copy(gate_hbm, gate, load_sem.at[0]),
        pltpu.make_async_copy(up_hbm, up, load_sem.at[1]),
        pltpu.make_async_copy(down_hbm, down, load_sem.at[2]),
        pltpu.make_async_copy(out_proj_hbm, out_proj, load_sem.at[3]),
        pltpu.make_async_copy(outgoing.at[me], arrived.at[me, tp], load_sem.at[4]),
        pltpu.make_async_copy(lat_own, lat_all.at[me_z, me_y, tp], load_sem.at[5]),
    ]
    for load in loads:
        load.start()

    def remote(src, dst, kind, step, device):
        return pltpu.make_async_remote_copy(
            src_ref=src,
            dst_ref=dst,
            send_sem=send_sem.at[kind, step],
            recv_sem=recv_sem.at[kind, step],
            device_id=device,
            device_id_type=pl.DeviceIdType.MESH,
        )

    def ahead(step):
        return (me_z + step // 2) % depth_z * 2 + (me_y + step) % 2

    def behind(step):
        return (me_z + depth_z - step // 2) % depth_z * 2 + (me_y + step) % 2

    below = (me_z + depth_z - 1) % depth_z * 2
    above = (me_z + 1) % depth_z * 2
    relay_peer = below + 1 - me_y
    relay_end = below + me_y
    relay_from = above + 1 - me_y

    barrier = pltpu.get_barrier_semaphore()

    def greet(step, carry):
        pl.semaphore_signal(
            barrier,
            inc=1,
            device_id={"ep": (me + step) % experts},
            device_id_type=pl.DeviceIdType.MESH,
        )
        return carry

    lax.fori_loop(1, experts, greet, 0)
    for peer in (mate, far, cross):
        pl.semaphore_signal(
            barrier, inc=1, device_id={"tp": peer}, device_id_type=pl.DeviceIdType.MESH
        )
    pl.semaphore_wait(barrier, experts + 2)

    def ep_rows(step, slot):
        target = ahead(step)
        return remote(outgoing.at[target], arrived.at[slot, tp], 0, step, {"ep": target})

    def rows_out():
        return remote(
            outgoing.at[ahead(middle)], relay_in, 0, middle, {"ep": relay_peer}
        )

    def rows_on(slot):
        return remote(relay_in, arrived.at[slot, tp], 12, middle, {"ep": relay_end})

    def back_out():
        return remote(
            result.at[behind(middle)], relay_back, 11, middle, {"ep": relay_peer}
        )

    def back_on(slot):
        return remote(relay_back, returned.at[slot], 13, middle, {"ep": relay_end})

    def lat_x(block):
        return remote(lat_own, lat_all.at[me_z, me_y, block], 5, 0, {"tp": far})

    def lat_z(shift, part, origin):
        block = (tp + 2 * part) % n_tp
        target = (me_z + shift) % depth_z * 2 + me_y
        return remote(
            lat_all.at[me_z, me_y, block],
            lat_all.at[origin, me_y, block],
            1,
            shift * 2 + part,
            {"ep": target},
        )

    def lat_y(part, side):
        place = lat_all.at[:, side, (tp + 2 * part) % n_tp]
        return remote(place, place, 3, part, {"ep": me_z * 2 + 1 - me_y})

    def lat_mate(part, first):
        place = lat_all.at[:, :, (first + 2 * part) % n_tp]
        return remote(place, place, 7, part, {"tp": mate})

    def hop_rows(kind, step, block, peer):
        source = behind(step)
        place = arrived.at[source, block]
        return remote(place, place, kind, step, {"tp": peer})

    def to_mate(kind, step, block, part):
        source = behind(step)
        return remote(
            partial.at[source, block], from_pair.at[source, part], kind, step, {"tp": mate}
        )

    def to_far(step):
        source = behind(step)
        return remote(pair_sum.at[source], from_far.at[source], 10, step, {"tp": far})

    def back(step, slot):
        source = behind(step)
        return remote(result.at[source], returned.at[slot], 11, step, {"ep": source})

    lat_x(tp).start()
    if middle < experts:
        rows_out().start()

    def send_rows(step, carry):
        @pl.when(step != middle)
        def _():
            ep_rows(step, me).start()

        return carry

    lax.fori_loop(1, experts, send_rows, 0)
    for load in loads[4:]:
        load.wait()

    def forward(step):
        source = behind(step)

        @pl.when((step > 0) & (step != middle))
        def _():
            ep_rows(step, source).wait_recv()

        if middle < experts:

            @pl.when(step == middle)
            def _():
                rows_on(source).wait_recv()

        hop_rows(4, step, tp, far).start()
        hop_rows(2, step, tp, mate).start()

    def relay(step):
        hop_rows(4, step, far, far).wait_recv()
        hop_rows(6, step, far, mate).start()

    def compute(step):
        source = behind(step)
        hop_rows(2, step, mate, mate).wait_recv()
        hop_rows(6, step, cross, mate).wait_recv()

        @pl.when(step == 0)
        def _():
            for load in loads[:3]:
                load.wait()

        rows = arrived[source].reshape(n_tp * capacity, width)
        gate_values = jnp.dot(rows, gate[...], preferred_element_type=jnp.float32)
        up_values = jnp.dot(rows, up[...], preferred_element_type=jnp.float32)
        hidden = (gate_values / (1.0 + jnp.exp(-gate_values)) * up_values).astype(jnp.bfloat16)
        product = jnp.dot(hidden, down[...], preferred_element_type=jnp.float32)
        partial[source] = product.astype(jnp.bfloat16).reshape(n_tp, capacity, width)
        to_mate(9, step, cross, 1).start()
        to_mate(8, step, mate, 0).start()

    def reduce_pair(step):
        source = behind(step)
        to_mate(9, step, cross, 1).wait_recv()
        pair_sum[source] = (
            partial[source, far].astype(jnp.float32) + from_pair[source, 1].astype(jnp.float32)
        ).astype(jnp.bfloat16)
        to_far(step).start()

    def reduce_far(step):
        source = behind(step)
        to_mate(8, step, mate, 0).wait_recv()
        to_far(step).wait_recv()
        result[source] = (
            partial[source, tp].astype(jnp.float32)
            + from_pair[source, 0].astype(jnp.float32)
            + from_far[source].astype(jnp.float32)
        ).astype(jnp.bfloat16)

        @pl.when((step > 0) & (step != middle))
        def _():
            back(step, me).start()

        if middle < experts:

            @pl.when(step == middle)
            def _():
                back_out().start()

        @pl.when(step == 0)
        def _():
            returned[me] = result[me]

    def attend():
        rows = query_big.shape[1]
        latent_width = key_up.shape[0]
        nope_width = key_up.shape[1]
        value_width = value_up.shape[1] // heads
        packed = lat_all[...].reshape(-1, lat_all.shape[-1])
        normed = packed[:, :latent_width]
        seq = packed.shape[0]
        keys[:, :nope_width] = jnp.dot(
            normed, key_up[...], preferred_element_type=jnp.float32
        ).astype(jnp.bfloat16)
        keys[:, nope_width:] = packed[:, latent_width:]
        values = jnp.dot(normed, value_up[...], preferred_element_type=jnp.float32).astype(
            jnp.bfloat16
        )
        query_pos = me * rows + lax.broadcasted_iota(jnp.int32, (rows, seq), 0)
        allowed = lax.broadcasted_iota(jnp.int32, (rows, seq), 1) <= query_pos
        lane = lax.broadcasted_iota(jnp.int32, (rows, heads * value_width), 1)
        scale = (nope_width // heads + rope_width) ** (-0.5)
        gathered = jnp.zeros((rows, heads * value_width), jnp.float32)
        for head in range(heads):
            scores = (
                lax.dot_general(
                    query_big[head],
                    keys[...],
                    (((1,), (1,)), ((), ())),
                    preferred_element_type=jnp.float32,
                )
                * scale
            )
            scores = jnp.where(allowed, scores, masked_value)
            raised = jnp.exp(scores - jnp.max(scores, axis=1, keepdims=True))
            totals = jnp.sum(raised, axis=1, keepdims=True)
            weighted = jnp.dot(
                raised.astype(jnp.bfloat16), values, preferred_element_type=jnp.float32
            )
            inside = (lane >= head * value_width) & (lane < (head + 1) * value_width)
            gathered = jnp.where(inside, weighted / totals, gathered)
        heads_own[...] = gathered.astype(jnp.bfloat16).reshape(heads_own.shape)

    def head_copy(number, peer, slot):
        return pltpu.make_async_remote_copy(
            src_ref=heads_own.at[peer],
            dst_ref=heads_all.at[slot],
            send_sem=head_send.at[number],
            recv_sem=head_recv.at[number],
            device_id={"tp": peer},
            device_id_type=pl.DeviceIdType.MESH,
        )

    def stage(turn, carry):
        @pl.when(turn < experts)
        def _():
            forward(turn)

        @pl.when((turn >= 1) & (turn < experts + 1))
        def _():
            relay(turn - 1)

        @pl.when((turn >= 2) & (turn < experts + 2))
        def _():
            compute(turn - 2)

        @pl.when((turn >= 3) & (turn < experts + 3))
        def _():
            reduce_pair(turn - 3)

        @pl.when(turn >= 4)
        def _():
            reduce_far(turn - 4)

        @pl.when(turn == 1)
        def _():
            lat_x(far).wait_recv()

            def spread(shift, inner):
                lat_z(shift, 0, me_z).start()
                lat_z(shift, 1, me_z).start()
                return inner

            lax.fori_loop(1, depth_z, spread, 0)

        @pl.when(turn == experts - 1)
        def _():
            def collect(shift, inner):
                origin = (me_z + depth_z - shift) % depth_z
                lat_z(shift, 0, origin).wait_recv()
                lat_z(shift, 1, origin).wait_recv()
                return inner

            lax.fori_loop(1, depth_z, collect, 0)
            lat_y(0, me_y).start()
            lat_y(1, me_y).start()

        @pl.when(turn == experts + 1)
        def _():
            lat_y(0, 1 - me_y).wait_recv()
            lat_y(1, 1 - me_y).wait_recv()
            lat_mate(0, tp).start()
            lat_mate(1, tp).start()

        if middle < experts:

            @pl.when(turn == 2)
            def _():
                rows_out().wait_recv()
                rows_on(relay_from).start()

        return carry

    lax.fori_loop(0, experts + 4, stage, 0)

    if middle < experts:
        back_out().wait_recv()
        back_on(relay_from).start()
    lat_mate(0, mate).wait_recv()
    lat_mate(1, mate).wait_recv()
    attend()
    peers = (mate, far, cross)
    for number, peer in enumerate(peers):
        head_copy(number, peer, tp).start()
    heads_all[tp] = heads_own[tp]
    loads[3].wait()
    for number, peer in enumerate(peers):
        head_copy(number, peer, peer).wait_recv()
    depth = heads_all.shape[2]
    total = jnp.zeros(mixed.shape, jnp.float32)
    for part in range(n_tp):
        total = total + jnp.dot(
            heads_all[part],
            out_proj[part * depth : (part + 1) * depth, :],
            preferred_element_type=jnp.float32,
        )
    mixed[...] = total.astype(mixed.dtype)

    def finish(step, carry):
        @pl.when(step != middle)
        def _():
            back(step, ahead(step)).wait_recv()

        if middle < experts:

            @pl.when(step == middle)
            def _():
                back_on(ahead(middle)).wait_recv()

        return carry

    lax.fori_loop(1, experts, finish, 0)

    answers = returned[...].reshape(experts * capacity, width)
    row = lax.broadcasted_iota(jnp.int32, (slots.shape[0], experts * capacity), 1)
    chosen = jnp.zeros(moe_out.shape, jnp.float32)
    for pick in range(slots.shape[1]):
        table = jnp.where(row == slots[:, pick : pick + 1], 1.0, 0.0).astype(jnp.bfloat16)
        chosen = chosen + shares[:, pick : pick + 1] * jnp.dot(
            table, answers, preferred_element_type=jnp.float32
        )
    moe_out[...] = chosen.astype(moe_out.dtype)

    def finish_ep(step, carry):
        @pl.when(step != middle)
        def _():
            ep_rows(step, me).wait_send()
            back(step, me).wait_send()

        return carry

    lax.fori_loop(1, experts, finish_ep, 0)
    if middle < experts:
        rows_out().wait_send()
        rows_on(relay_from).wait_send()
        back_out().wait_send()
        back_on(relay_from).wait_send()
    lat_x(tp).wait_send()

    def finish_lat(shift, carry):
        lat_z(shift, 0, me_z).wait_send()
        lat_z(shift, 1, me_z).wait_send()
        return carry

    lax.fori_loop(1, depth_z, finish_lat, 0)
    for part in range(2):
        lat_y(part, me_y).wait_send()
        lat_mate(part, tp).wait_send()

    def finish_tp(step, carry):
        hop_rows(4, step, tp, far).wait_send()
        hop_rows(2, step, tp, mate).wait_send()
        hop_rows(6, step, far, mate).wait_send()
        to_mate(9, step, cross, 1).wait_send()
        to_mate(8, step, mate, 0).wait_send()
        to_far(step).wait_send()
        return carry

    lax.fori_loop(0, experts, finish_tp, 0)
    for number, peer in enumerate(peers):
        head_copy(number, peer, tp).wait_send()


def padded(amount):
    return -(-amount // 128) * 128


def fused_body(
    query,
    latent,
    rope_key,
    latent_gain,
    key_up,
    value_up,
    out_proj,
    tokens,
    moe_gain,
    routes,
    group_prob,
    expert_prob,
    w_gate,
    w_up,
    w_down,
):
    n_ep = lax.axis_size("ep")
    n_tp = lax.axis_size("tp")
    query_rows = query.shape[0]
    own_rows, latent_width = latent.shape
    query_start = lax.axis_index("ep") * query_rows
    key_start = query_start + lax.axis_index("tp") * own_rows
    heads = query.shape[1] // (NOPE + ROPE_DIM)
    normed_latent = rms_scale(latent, latent_gain).astype(jnp.bfloat16)
    key_cos, key_sin = tables(key_start + jnp.arange(own_rows, dtype=jnp.int32), ROPE_DIM)
    rotated_key = rotate(rope_key.astype(jnp.float32), key_cos, key_sin).astype(jnp.bfloat16)
    rope_room = padded(ROPE_DIM)
    gap = rope_room - ROPE_DIM
    lat_own = jnp.concatenate([normed_latent, jnp.pad(rotated_key, ((0, 0), (0, gap)))], axis=1)
    query_cos, query_sin = tables(query_start + jnp.arange(query_rows, dtype=jnp.int32), ROPE_DIM)
    query_heads = query.reshape(query_rows, heads, NOPE + ROPE_DIM).transpose(1, 0, 2)
    turned = rotate(
        query_heads[..., NOPE:].astype(jnp.float32), query_cos[None], query_sin[None]
    ).astype(jnp.bfloat16)
    own_head = jnp.eye(heads, dtype=jnp.bool_)[:, None, :, None]
    spread = jnp.where(own_head, query_heads[:, :, None, :NOPE], jnp.bfloat16(0)).reshape(
        heads, query_rows, heads * NOPE
    )
    query_big = jnp.concatenate(
        [spread, jnp.pad(turned, ((0, 0), (0, 0), (0, gap)))], axis=-1
    )

    row_count, width = tokens.shape
    top_count = routes.shape[1]
    capacity = 2 * top_count * row_count // n_ep
    normed = rms_scale(tokens, moe_gain).astype(jnp.bfloat16)
    flat_routes = routes.reshape(-1)
    onehot = (flat_routes[:, None] == jnp.arange(n_ep, dtype=jnp.int32)[None, :]).astype(jnp.int32)
    earlier = jnp.cumsum(onehot, axis=0) - onehot
    slot_index = jnp.sum(earlier * onehot, axis=1)
    target = flat_routes * capacity + slot_index
    owner = target[None, :] == jnp.arange(n_ep * capacity, dtype=jnp.int32)[:, None]
    dispatch_table = jnp.any(owner.reshape(n_ep * capacity, row_count, top_count), axis=2).astype(
        jnp.bfloat16
    )
    outgoing = jnp.dot(dispatch_table, normed, preferred_element_type=jnp.float32).astype(
        jnp.bfloat16
    )
    outgoing = outgoing.reshape(n_ep, capacity, width)

    shares = group_prob[:, None] * expert_prob / jnp.sum(expert_prob, axis=1, keepdims=True)
    bf16 = jnp.bfloat16
    lat_width = latent_width + rope_room
    vmem = pl.BlockSpec(memory_space=pltpu.VMEM)
    anywhere = pl.BlockSpec(memory_space=pl.ANY)
    mixed, moe_out = pl.pallas_call(
        functools.partial(both_halves, heads, ROPE_DIM),
        out_shape=(
            jax.ShapeDtypeStruct((own_rows, out_proj.shape[1]), bf16),
            jax.ShapeDtypeStruct((row_count, width), bf16),
        ),
        in_specs=[vmem] * 5 + [anywhere] * 4 + [vmem] * 2,
        out_specs=(vmem, vmem),
        scratch_shapes=[
            pltpu.VMEM((n_ep, capacity, width), bf16),
            pltpu.VMEM((capacity, width), bf16),
            pltpu.VMEM((capacity, width), bf16),
            pltpu.VMEM((n_ep, n_tp, capacity, width), bf16),
            pltpu.VMEM((n_ep // 2, 2, n_tp, own_rows, lat_width), bf16),
            pltpu.VMEM((n_ep, n_tp, capacity, width), bf16),
            pltpu.VMEM((n_ep, 2, capacity, width), bf16),
            pltpu.VMEM((n_ep, capacity, width), bf16),
            pltpu.VMEM((n_ep, capacity, width), bf16),
            pltpu.VMEM((n_ep, capacity, width), bf16),
            pltpu.VMEM((n_ep * n_tp * own_rows, key_up.shape[1] + rope_room), bf16),
            pltpu.VMEM((n_tp, own_rows, value_up.shape[1]), bf16),
            pltpu.VMEM((n_tp, own_rows, value_up.shape[1]), bf16),
            pltpu.VMEM(out_proj.shape, bf16),
            pltpu.VMEM(w_gate.shape[1:], bf16),
            pltpu.VMEM(w_up.shape[1:], bf16),
            pltpu.VMEM(w_down.shape[1:], bf16),
            pltpu.SemaphoreType.DMA((6,)),
            pltpu.SemaphoreType.DMA((14, n_ep)),
            pltpu.SemaphoreType.DMA((14, n_ep)),
            pltpu.SemaphoreType.DMA((3,)),
            pltpu.SemaphoreType.DMA((3,)),
        ],
        compiler_params=pltpu.CompilerParams(
            collective_id=0, has_side_effects=True, vmem_limit_bytes=56 * 1024 * 1024
        ),
        name="both_halves",
    )(
        outgoing,
        lat_own,
        query_big,
        key_up,
        value_up,
        out_proj,
        w_gate[0],
        w_up[0],
        w_down[0],
        target.reshape(row_count, top_count),
        shares,
    )
    return (mixed, moe_out)


def fits_kernel(mesh, *arrays):
    n_ep, n_tp = mesh.shape["ep"], mesh.shape["tp"]
    tokens, routes, latent = arrays[7], arrays[9], arrays[1]
    capacity = 2 * routes.shape[1] * tokens.shape[0] // (n_ep * n_tp) // n_ep
    own_rows = latent.shape[0] // (n_ep * n_tp)
    packed = latent.shape[0] <= 2048
    return n_tp == 4 and n_ep >= 8 and n_ep % 2 == 0 and capacity % 16 == 0 and own_rows % 16 == 0 and packed


def mapped(mesh, chosen):
    return jax.shard_map(
        chosen,
        mesh=mesh,
        in_specs=(
            P("ep", "tp"),
            P(("ep", "tp"), None),
            P(("ep", "tp"), None),
            P(),
            P(None, "tp"),
            P(None, "tp"),
            P(),
            P(("ep", "tp"), None),
            P(),
            P(("ep", "tp"), None),
            P(("ep", "tp")),
            P(("ep", "tp"), None),
            P("ep", None, "tp"),
            P("ep", None, "tp"),
            P("ep", "tp", None),
        ),
        out_specs=(P(("ep", "tp"), None), P(("ep", "tp"), None)),
        check_vma=False,
    )


def solution(mesh):
    def whole(*arrays):
        chosen = fused_body if fits_kernel(mesh, *arrays) else body
        return mapped(mesh, chosen)(*arrays)

    return whole
```

```python
import functools
import math

import jax
import jax.numpy as jnp
from jax import lax
from jax.experimental import pallas as pl
from jax.experimental.pallas import tpu as pltpu
from jax.sharding import PartitionSpec as P

NOPE = 64
ROPE_DIM = 32
V_DIM = 64


epsilon = 1e-06
rope_base = 10000.0
masked_value = -1e30


def rms_scale(values, gain):
    widened = values.astype(jnp.float32)
    return widened * lax.rsqrt(jnp.mean(widened * widened, axis=-1, keepdims=True) + epsilon) * gain


def tables(positions, rope_width):
    half_width = rope_width // 2
    inverse = rope_base ** (-2.0 * jnp.arange(half_width, dtype=jnp.float32) / rope_width)
    angles = positions.astype(jnp.float32)[:, None] * inverse[None, :]
    return (jnp.cos(angles), jnp.sin(angles))


def rotate(values, cosine, sine):
    half_width = values.shape[-1] // 2
    lower = values[..., :half_width]
    upper = values[..., half_width:]
    return jnp.concatenate([lower * cosine - upper * sine, lower * sine + upper * cosine], axis=-1)


def keep_state(state_in):
    return state_in


def attend_block(running, query_rot, query_pos, key_part, value_part, rope_part):
    amount = key_part.shape[0]
    span_rows = math.gcd(amount, 1024)
    head_count = query_rot.shape[1]
    scale_factor = query_rot.shape[2] ** (-0.5)
    last_query = query_pos[-1]

    def update(state, block_at):
        row_begin = block_at * span_rows
        keys_here = lax.dynamic_slice_in_dim(key_part, row_begin, span_rows, 0).reshape(
            span_rows, head_count, -1
        )
        values_here = lax.dynamic_slice_in_dim(value_part, row_begin, span_rows, 0).reshape(
            span_rows, head_count, -1
        )
        rope_here = lax.dynamic_slice_in_dim(rope_part, row_begin, span_rows, 0)
        key_pos = row_begin + jnp.arange(span_rows, dtype=jnp.int32)

        def advance(state_in):
            top_old, totals, weighted = state_in
            shared = jnp.broadcast_to(
                rope_here[:, None, :], (span_rows, head_count, rope_here.shape[1])
            )
            full_keys = jnp.concatenate([keys_here, shared], axis=-1)
            scores = (
                jnp.einsum("qhd,khd->hqk", query_rot, full_keys, preferred_element_type=jnp.float32)
                * scale_factor
            )
            allowed = key_pos[None, :] <= query_pos[:, None]
            scores = jnp.where(allowed[None], scores, masked_value)
            top_new = jnp.maximum(top_old, jnp.max(scores, axis=-1))
            raised = jnp.where(allowed[None], jnp.exp(scores - top_new[..., None]), 0.0)
            factor = jnp.exp(top_old - top_new)
            totals = totals * factor + jnp.sum(raised, axis=-1)
            weighted = weighted * factor[..., None] + jnp.einsum(
                "hqk,khd->hqd",
                raised.astype(jnp.bfloat16),
                values_here,
                preferred_element_type=jnp.float32,
            )
            return (top_new, totals, weighted)

        return (lax.cond(key_pos[0] <= last_query, advance, keep_state, state), None)

    running, _ = lax.scan(update, running, jnp.arange(amount // span_rows))
    return running


def mixer_half(query, latent, rope_key, latent_gain, key_up, value_up, out_proj):
    query_rows = query.shape[0]
    own_rows = latent.shape[0]
    query_start = lax.axis_index("ep") * query_rows
    key_start = query_start + lax.axis_index("tp") * own_rows
    head_count = query.shape[1] // (NOPE + ROPE_DIM)
    normed = rms_scale(latent, latent_gain).astype(jnp.bfloat16)
    key_cos, key_sin = tables(key_start + jnp.arange(own_rows, dtype=jnp.int32), ROPE_DIM)
    rotated_key = rotate(rope_key.astype(jnp.float32), key_cos, key_sin).astype(jnp.bfloat16)
    query_pos = query_start + jnp.arange(query_rows, dtype=jnp.int32)
    query_cos, query_sin = tables(query_pos, ROPE_DIM)
    query_heads = query.reshape(query_rows, head_count, NOPE + ROPE_DIM)
    turned = rotate(
        query_heads[..., NOPE:].astype(jnp.float32), query_cos[:, None, :], query_sin[:, None, :]
    ).astype(jnp.bfloat16)
    query_rot = jnp.concatenate([query_heads[..., :NOPE], turned], axis=-1)
    last_query = query_start + query_rows - 1
    initial = (
        jnp.full((head_count, query_rows), masked_value, jnp.float32),
        jnp.zeros((head_count, query_rows), jnp.float32),
        jnp.zeros((head_count, query_rows, V_DIM), jnp.float32),
    )
    shard_rows = (
        lax.all_gather(normed, ("ep", "tp"), axis=0, tiled=True),
        lax.all_gather(rotated_key, ("ep", "tp"), axis=0, tiled=True),
    )

    def compute(state_in):
        key_part = jnp.dot(shard_rows[0], key_up, preferred_element_type=jnp.float32).astype(
            jnp.bfloat16
        )
        value_part = jnp.dot(shard_rows[0], value_up, preferred_element_type=jnp.float32).astype(
            jnp.bfloat16
        )
        return attend_block(state_in, query_rot, query_pos, key_part, value_part, shard_rows[1])

    running = lax.cond(jnp.int32(0) <= last_query, compute, keep_state, initial)
    totals = running[1]
    weighted = running[2]
    attention = (
        (weighted / totals[..., None])
        .transpose(1, 0, 2)
        .reshape(query_rows, head_count * V_DIM)
        .astype(jnp.bfloat16)
    )
    own_attention = lax.all_to_all(attention, "tp", split_axis=0, concat_axis=1, tiled=True)
    return jnp.dot(own_attention, out_proj, preferred_element_type=jnp.float32).astype(jnp.bfloat16)


def expert_half(tokens, moe_gain, routes, group_prob, expert_prob, w_gate, w_up, w_down):
    row_count, model_width = tokens.shape
    top_count = routes.shape[1]
    expert_count = lax.axis_size("ep")
    capacity = 2 * top_count * row_count // expert_count
    normed = rms_scale(tokens, moe_gain).astype(jnp.bfloat16)
    flat_routes = routes.reshape(-1)
    onehot = (flat_routes[:, None] == jnp.arange(expert_count, dtype=jnp.int32)[None, :]).astype(
        jnp.int32
    )
    earlier = jnp.cumsum(onehot, axis=0) - onehot
    slot_index = jnp.sum(earlier * onehot, axis=1)
    target = flat_routes * capacity + slot_index
    owner = target[None, :] == jnp.arange(expert_count * capacity, dtype=jnp.int32)[:, None]
    dispatch_table = jnp.any(
        owner.reshape(expert_count * capacity, row_count, top_count), axis=2
    ).astype(jnp.bfloat16)
    outgoing = jnp.dot(dispatch_table, normed, preferred_element_type=jnp.float32).astype(
        jnp.bfloat16
    )
    outgoing = outgoing.reshape(expert_count, capacity, model_width)
    arrived = lax.all_to_all(outgoing, "ep", split_axis=0, concat_axis=0, tiled=True)
    sources, slots, _ = arrived.shape
    flat_rows = arrived.reshape(sources * slots, model_width)
    shard_rows = lax.all_gather(flat_rows, "tp", axis=0, tiled=True)
    gate_values = jnp.dot(shard_rows, w_gate[0], preferred_element_type=jnp.float32)
    up_values = jnp.dot(shard_rows, w_up[0], preferred_element_type=jnp.float32)
    hidden = (jax.nn.silu(gate_values) * up_values).astype(jnp.bfloat16)

    def lower(offset, amount):
        return jnp.dot(hidden, w_down[0], preferred_element_type=jnp.float32)

    summed = lax.psum_scatter(
        lower(jnp.int32(0), sources * slots * lax.axis_size("tp")).astype(jnp.bfloat16),
        "tp",
        scatter_dimension=0,
        tiled=True,
    )
    result = summed.reshape(sources, slots, model_width)
    returned = lax.all_to_all(result, "ep", split_axis=0, concat_axis=0, tiled=True)
    returned_flat = returned.reshape(expert_count * capacity, model_width)
    picked = returned_flat[target].reshape(row_count, top_count, model_width).astype(jnp.float32)
    shares = group_prob[:, None] * expert_prob / jnp.sum(expert_prob, axis=1, keepdims=True)
    return jnp.sum(shares[:, :, None] * picked, axis=1).astype(jnp.bfloat16)


def body(
    query,
    latent,
    rope_key,
    latent_gain,
    key_up,
    value_up,
    out_proj,
    tokens,
    moe_gain,
    routes,
    group_prob,
    expert_prob,
    w_gate,
    w_up,
    w_down,
):
    mixed = mixer_half(query, latent, rope_key, latent_gain, key_up, value_up, out_proj)
    moe_out = expert_half(tokens, moe_gain, routes, group_prob, expert_prob, w_gate, w_up, w_down)
    return (mixed, moe_out)


def both_halves(
    heads,
    rope_width,
    outgoing,
    lat_own,
    query_big,
    key_up,
    value_up,
    out_proj_hbm,
    gate_hbm,
    up_hbm,
    down_hbm,
    slots,
    shares,
    mixed,
    moe_out,
    returned,
    relay_in,
    relay_back,
    arrived,
    lat_all,
    partial,
    from_pair,
    pair_sum,
    from_far,
    result,
    keys,
    heads_own,
    heads_all,
    out_proj,
    gate,
    up,
    down,
    load_sem,
    send_sem,
    recv_sem,
    head_send,
    head_recv,
):
    experts, capacity, width = outgoing.shape
    n_tp = lat_all.shape[2]
    depth_z = experts // 2
    middle = depth_z + 1 if depth_z == 4 else experts
    me = lax.axis_index("ep")
    tp = lax.axis_index("tp")
    me_z = me // 2
    me_y = me % 2
    mate = tp + 1 - 2 * (tp % 2)
    far = (tp + 2) % n_tp
    cross = (mate + 2) % n_tp

    loads = [
        pltpu.make_async_copy(gate_hbm, gate, load_sem.at[0]),
        pltpu.make_async_copy(up_hbm, up, load_sem.at[1]),
        pltpu.make_async_copy(down_hbm, down, load_sem.at[2]),
        pltpu.make_async_copy(out_proj_hbm, out_proj, load_sem.at[3]),
        pltpu.make_async_copy(outgoing.at[me], arrived.at[me, tp], load_sem.at[4]),
        pltpu.make_async_copy(lat_own, lat_all.at[me_z, me_y, tp], load_sem.at[5]),
    ]
    for load in loads:
        load.start()

    def remote(src, dst, kind, step, device):
        return pltpu.make_async_remote_copy(
            src_ref=src,
            dst_ref=dst,
            send_sem=send_sem.at[kind, step],
            recv_sem=recv_sem.at[kind, step],
            device_id=device,
            device_id_type=pl.DeviceIdType.MESH,
        )

    def ahead(step):
        return (me_z + step // 2) % depth_z * 2 + (me_y + step) % 2

    def behind(step):
        return (me_z + depth_z - step // 2) % depth_z * 2 + (me_y + step) % 2

    below = (me_z + depth_z - 1) % depth_z * 2
    above = (me_z + 1) % depth_z * 2
    relay_peer = below + 1 - me_y
    relay_end = below + me_y
    relay_from = above + 1 - me_y

    barrier = pltpu.get_barrier_semaphore()

    def greet(step, carry):
        pl.semaphore_signal(
            barrier,
            inc=1,
            device_id={"ep": (me + step) % experts},
            device_id_type=pl.DeviceIdType.MESH,
        )
        return carry

    lax.fori_loop(1, experts, greet, 0)
    for peer in (mate, far, cross):
        pl.semaphore_signal(
            barrier, inc=1, device_id={"tp": peer}, device_id_type=pl.DeviceIdType.MESH
        )
    pl.semaphore_wait(barrier, experts + 2)

    def ep_rows(step, slot):
        target = ahead(step)
        return remote(outgoing.at[target], arrived.at[slot, tp], 0, step, {"ep": target})

    def rows_out():
        return remote(
            outgoing.at[ahead(middle)], relay_in, 0, middle, {"ep": relay_peer}
        )

    def rows_on(slot):
        return remote(relay_in, arrived.at[slot, tp], 12, middle, {"ep": relay_end})

    def back_out():
        return remote(
            result.at[behind(middle)], relay_back, 11, middle, {"ep": relay_peer}
        )

    def back_on(slot):
        return remote(relay_back, returned.at[slot], 13, middle, {"ep": relay_end})

    def lat_x(block):
        return remote(lat_own, lat_all.at[me_z, me_y, block], 5, 0, {"tp": far})

    def lat_z(shift, part, origin):
        block = (tp + 2 * part) % n_tp
        target = (me_z + shift) % depth_z * 2 + me_y
        return remote(
            lat_all.at[me_z, me_y, block],
            lat_all.at[origin, me_y, block],
            1,
            shift * 2 + part,
            {"ep": target},
        )

    def lat_y(part, side):
        place = lat_all.at[:, side, (tp + 2 * part) % n_tp]
        return remote(place, place, 3, part, {"ep": me_z * 2 + 1 - me_y})

    def lat_mate(part, first):
        place = lat_all.at[:, :, (first + 2 * part) % n_tp]
        return remote(place, place, 7, part, {"tp": mate})

    def hop_rows(kind, step, block, peer):
        source = behind(step)
        place = arrived.at[source, block]
        return remote(place, place, kind, step, {"tp": peer})

    def to_mate(kind, step, block, part):
        source = behind(step)
        return remote(
            partial.at[source, block], from_pair.at[source, part], kind, step, {"tp": mate}
        )

    def to_far(step):
        source = behind(step)
        return remote(pair_sum.at[source], from_far.at[source], 10, step, {"tp": far})

    def back(step, slot):
        source = behind(step)
        return remote(result.at[source], returned.at[slot], 11, step, {"ep": source})

    lat_x(tp).start()
    if middle < experts:
        rows_out().start()

    def send_rows(step, carry):
        @pl.when(step != middle)
        def _():
            ep_rows(step, me).start()

        return carry

    lax.fori_loop(1, experts, send_rows, 0)
    for load in loads[4:]:
        load.wait()

    def forward(step):
        source = behind(step)

        @pl.when((step > 0) & (step != middle))
        def _():
            ep_rows(step, source).wait_recv()

        if middle < experts:

            @pl.when(step == middle)
            def _():
                rows_on(source).wait_recv()

        hop_rows(4, step, tp, far).start()
        hop_rows(2, step, tp, mate).start()

    def relay(step):
        hop_rows(4, step, far, far).wait_recv()
        hop_rows(6, step, far, mate).start()

    def compute(step):
        source = behind(step)
        hop_rows(2, step, mate, mate).wait_recv()
        hop_rows(6, step, cross, mate).wait_recv()

        @pl.when(step == 0)
        def _():
            for load in loads[:3]:
                load.wait()

        rows = arrived[source].reshape(n_tp * capacity, width)
        gate_values = jnp.dot(rows, gate[...], preferred_element_type=jnp.float32)
        up_values = jnp.dot(rows, up[...], preferred_element_type=jnp.float32)
        hidden = (gate_values / (1.0 + jnp.exp(-gate_values)) * up_values).astype(jnp.bfloat16)
        product = jnp.dot(hidden, down[...], preferred_element_type=jnp.float32)
        partial[source] = product.astype(jnp.bfloat16).reshape(n_tp, capacity, width)
        to_mate(9, step, cross, 1).start()
        to_mate(8, step, mate, 0).start()

    def reduce_pair(step):
        source = behind(step)
        to_mate(9, step, cross, 1).wait_recv()
        pair_sum[source] = (
            partial[source, far].astype(jnp.float32) + from_pair[source, 1].astype(jnp.float32)
        ).astype(jnp.bfloat16)
        to_far(step).start()

    def reduce_far(step):
        source = behind(step)
        to_mate(8, step, mate, 0).wait_recv()
        to_far(step).wait_recv()
        result[source] = (
            partial[source, tp].astype(jnp.float32)
            + from_pair[source, 0].astype(jnp.float32)
            + from_far[source].astype(jnp.float32)
        ).astype(jnp.bfloat16)

        @pl.when((step > 0) & (step != middle))
        def _():
            back(step, me).start()

        if middle < experts:

            @pl.when(step == middle)
            def _():
                back_out().start()

        @pl.when(step == 0)
        def _():
            returned[me] = result[me]

    def attend():
        rows = query_big.shape[1]
        latent_width = key_up.shape[0]
        nope_width = key_up.shape[1]
        value_width = value_up.shape[1] // heads
        packed = lat_all[...].reshape(-1, lat_all.shape[-1])
        normed = packed[:, :latent_width]
        seq = packed.shape[0]
        keys[:, :nope_width] = jnp.dot(
            normed, key_up[...], preferred_element_type=jnp.float32
        ).astype(jnp.bfloat16)
        keys[:, nope_width:] = packed[:, latent_width:]
        values = jnp.dot(normed, value_up[...], preferred_element_type=jnp.float32).astype(
            jnp.bfloat16
        )
        query_pos = me * rows + lax.broadcasted_iota(jnp.int32, (rows, seq), 0)
        allowed = lax.broadcasted_iota(jnp.int32, (rows, seq), 1) <= query_pos
        lane = lax.broadcasted_iota(jnp.int32, (rows, heads * value_width), 1)
        scale = (nope_width // heads + rope_width) ** (-0.5)
        gathered = jnp.zeros((rows, heads * value_width), jnp.float32)
        for head in range(heads):
            scores = (
                lax.dot_general(
                    query_big[head],
                    keys[...],
                    (((1,), (1,)), ((), ())),
                    preferred_element_type=jnp.float32,
                )
                * scale
            )
            scores = jnp.where(allowed, scores, masked_value)
            raised = jnp.exp(scores - jnp.max(scores, axis=1, keepdims=True))
            totals = jnp.sum(raised, axis=1, keepdims=True)
            weighted = jnp.dot(
                raised.astype(jnp.bfloat16), values, preferred_element_type=jnp.float32
            )
            inside = (lane >= head * value_width) & (lane < (head + 1) * value_width)
            gathered = jnp.where(inside, weighted / totals, gathered)
        heads_own[...] = gathered.astype(jnp.bfloat16).reshape(heads_own.shape)

    def head_copy(number, peer, slot):
        return pltpu.make_async_remote_copy(
            src_ref=heads_own.at[peer],
            dst_ref=heads_all.at[slot],
            send_sem=head_send.at[number],
            recv_sem=head_recv.at[number],
            device_id={"tp": peer},
            device_id_type=pl.DeviceIdType.MESH,
        )

    def stage(turn, carry):
        @pl.when(turn >= 4)
        def _():
            reduce_far(turn - 4)

        @pl.when((turn >= 3) & (turn < experts + 3))
        def _():
            reduce_pair(turn - 3)

        @pl.when((turn >= 2) & (turn < experts + 2))
        def _():
            compute(turn - 2)

        @pl.when((turn >= 1) & (turn < experts + 1))
        def _():
            relay(turn - 1)

        @pl.when(turn < experts)
        def _():
            forward(turn)

        @pl.when(turn == 1)
        def _():
            lat_x(far).wait_recv()

            def spread(shift, inner):
                lat_z(shift, 0, me_z).start()
                lat_z(shift, 1, me_z).start()
                return inner

            lax.fori_loop(1, depth_z, spread, 0)

        @pl.when(turn == experts - 1)
        def _():
            def collect(shift, inner):
                origin = (me_z + depth_z - shift) % depth_z
                lat_z(shift, 0, origin).wait_recv()
                lat_z(shift, 1, origin).wait_recv()
                return inner

            lax.fori_loop(1, depth_z, collect, 0)
            lat_y(0, me_y).start()
            lat_y(1, me_y).start()

        @pl.when(turn == experts + 1)
        def _():
            lat_y(0, 1 - me_y).wait_recv()
            lat_y(1, 1 - me_y).wait_recv()
            lat_mate(0, tp).start()
            lat_mate(1, tp).start()

        if middle < experts:

            @pl.when(turn == 2)
            def _():
                rows_out().wait_recv()
                rows_on(relay_from).start()

        if middle < experts:

            @pl.when(turn == experts + 2)
            def _():
                back_out().wait_recv()
                back_on(relay_from).start()

        return carry

    lax.fori_loop(0, experts + 4, stage, 0)

    lat_mate(0, mate).wait_recv()
    lat_mate(1, mate).wait_recv()
    attend()
    peers = (mate, far, cross)
    for number, peer in enumerate(peers):
        head_copy(number, peer, tp).start()
    heads_all[tp] = heads_own[tp]
    loads[3].wait()
    for number, peer in enumerate(peers):
        head_copy(number, peer, peer).wait_recv()
    depth = heads_all.shape[2]
    total = jnp.zeros(mixed.shape, jnp.float32)
    for part in range(n_tp):
        total = total + jnp.dot(
            heads_all[part],
            out_proj[part * depth : (part + 1) * depth, :],
            preferred_element_type=jnp.float32,
        )
    mixed[...] = total.astype(mixed.dtype)

    def finish(step, carry):
        @pl.when(step != middle)
        def _():
            back(step, ahead(step)).wait_recv()

        if middle < experts:

            @pl.when(step == middle)
            def _():
                back_on(ahead(middle)).wait_recv()

        return carry

    lax.fori_loop(1, experts, finish, 0)

    answers = returned[...].reshape(experts * capacity, width)
    row = lax.broadcasted_iota(jnp.int32, (slots.shape[0], experts * capacity), 1)
    chosen = jnp.zeros(moe_out.shape, jnp.float32)
    for pick in range(slots.shape[1]):
        table = jnp.where(row == slots[:, pick : pick + 1], 1.0, 0.0).astype(jnp.bfloat16)
        chosen = chosen + shares[:, pick : pick + 1] * jnp.dot(
            table, answers, preferred_element_type=jnp.float32
        )
    moe_out[...] = chosen.astype(moe_out.dtype)

    def finish_ep(step, carry):
        @pl.when(step != middle)
        def _():
            ep_rows(step, me).wait_send()
            back(step, me).wait_send()

        return carry

    lax.fori_loop(1, experts, finish_ep, 0)
    if middle < experts:
        rows_out().wait_send()
        rows_on(relay_from).wait_send()
        back_out().wait_send()
        back_on(relay_from).wait_send()
    lat_x(tp).wait_send()

    def finish_lat(shift, carry):
        lat_z(shift, 0, me_z).wait_send()
        lat_z(shift, 1, me_z).wait_send()
        return carry

    lax.fori_loop(1, depth_z, finish_lat, 0)
    for part in range(2):
        lat_y(part, me_y).wait_send()
        lat_mate(part, tp).wait_send()

    def finish_tp(step, carry):
        hop_rows(4, step, tp, far).wait_send()
        hop_rows(2, step, tp, mate).wait_send()
        hop_rows(6, step, far, mate).wait_send()
        to_mate(9, step, cross, 1).wait_send()
        to_mate(8, step, mate, 0).wait_send()
        to_far(step).wait_send()
        return carry

    lax.fori_loop(0, experts, finish_tp, 0)
    for number, peer in enumerate(peers):
        head_copy(number, peer, tp).wait_send()


def padded(amount):
    return -(-amount // 128) * 128


def fused_body(
    query,
    latent,
    rope_key,
    latent_gain,
    key_up,
    value_up,
    out_proj,
    tokens,
    moe_gain,
    routes,
    group_prob,
    expert_prob,
    w_gate,
    w_up,
    w_down,
):
    n_ep = lax.axis_size("ep")
    n_tp = lax.axis_size("tp")
    query_rows = query.shape[0]
    own_rows, latent_width = latent.shape
    query_start = lax.axis_index("ep") * query_rows
    key_start = query_start + lax.axis_index("tp") * own_rows
    heads = query.shape[1] // (NOPE + ROPE_DIM)
    normed_latent = rms_scale(latent, latent_gain).astype(jnp.bfloat16)
    key_cos, key_sin = tables(key_start + jnp.arange(own_rows, dtype=jnp.int32), ROPE_DIM)
    rotated_key = rotate(rope_key.astype(jnp.float32), key_cos, key_sin).astype(jnp.bfloat16)
    rope_room = padded(ROPE_DIM)
    gap = rope_room - ROPE_DIM
    lat_own = jnp.concatenate([normed_latent, jnp.pad(rotated_key, ((0, 0), (0, gap)))], axis=1)
    query_cos, query_sin = tables(query_start + jnp.arange(query_rows, dtype=jnp.int32), ROPE_DIM)
    query_heads = query.reshape(query_rows, heads, NOPE + ROPE_DIM).transpose(1, 0, 2)
    turned = rotate(
        query_heads[..., NOPE:].astype(jnp.float32), query_cos[None], query_sin[None]
    ).astype(jnp.bfloat16)
    own_head = jnp.eye(heads, dtype=jnp.bool_)[:, None, :, None]
    spread = jnp.where(own_head, query_heads[:, :, None, :NOPE], jnp.bfloat16(0)).reshape(
        heads, query_rows, heads * NOPE
    )
    query_big = jnp.concatenate(
        [spread, jnp.pad(turned, ((0, 0), (0, 0), (0, gap)))], axis=-1
    )

    row_count, width = tokens.shape
    top_count = routes.shape[1]
    capacity = 2 * top_count * row_count // n_ep
    normed = rms_scale(tokens, moe_gain).astype(jnp.bfloat16)
    flat_routes = routes.reshape(-1)
    onehot = (flat_routes[:, None] == jnp.arange(n_ep, dtype=jnp.int32)[None, :]).astype(jnp.int32)
    earlier = jnp.cumsum(onehot, axis=0) - onehot
    slot_index = jnp.sum(earlier * onehot, axis=1)
    target = flat_routes * capacity + slot_index
    owner = target[None, :] == jnp.arange(n_ep * capacity, dtype=jnp.int32)[:, None]
    dispatch_table = jnp.any(owner.reshape(n_ep * capacity, row_count, top_count), axis=2).astype(
        jnp.bfloat16
    )
    outgoing = jnp.dot(dispatch_table, normed, preferred_element_type=jnp.float32).astype(
        jnp.bfloat16
    )
    outgoing = outgoing.reshape(n_ep, capacity, width)

    shares = group_prob[:, None] * expert_prob / jnp.sum(expert_prob, axis=1, keepdims=True)
    bf16 = jnp.bfloat16
    lat_width = latent_width + rope_room
    vmem = pl.BlockSpec(memory_space=pltpu.VMEM)
    anywhere = pl.BlockSpec(memory_space=pl.ANY)
    mixed, moe_out = pl.pallas_call(
        functools.partial(both_halves, heads, ROPE_DIM),
        out_shape=(
            jax.ShapeDtypeStruct((own_rows, out_proj.shape[1]), bf16),
            jax.ShapeDtypeStruct((row_count, width), bf16),
        ),
        in_specs=[vmem] * 5 + [anywhere] * 4 + [vmem] * 2,
        out_specs=(vmem, vmem),
        scratch_shapes=[
            pltpu.VMEM((n_ep, capacity, width), bf16),
            pltpu.VMEM((capacity, width), bf16),
            pltpu.VMEM((capacity, width), bf16),
            pltpu.VMEM((n_ep, n_tp, capacity, width), bf16),
            pltpu.VMEM((n_ep // 2, 2, n_tp, own_rows, lat_width), bf16),
            pltpu.VMEM((n_ep, n_tp, capacity, width), bf16),
            pltpu.VMEM((n_ep, 2, capacity, width), bf16),
            pltpu.VMEM((n_ep, capacity, width), bf16),
            pltpu.VMEM((n_ep, capacity, width), bf16),
            pltpu.VMEM((n_ep, capacity, width), bf16),
            pltpu.VMEM((n_ep * n_tp * own_rows, key_up.shape[1] + rope_room), bf16),
            pltpu.VMEM((n_tp, own_rows, value_up.shape[1]), bf16),
            pltpu.VMEM((n_tp, own_rows, value_up.shape[1]), bf16),
            pltpu.VMEM(out_proj.shape, bf16),
            pltpu.VMEM(w_gate.shape[1:], bf16),
            pltpu.VMEM(w_up.shape[1:], bf16),
            pltpu.VMEM(w_down.shape[1:], bf16),
            pltpu.SemaphoreType.DMA((6,)),
            pltpu.SemaphoreType.DMA((14, n_ep)),
            pltpu.SemaphoreType.DMA((14, n_ep)),
            pltpu.SemaphoreType.DMA((3,)),
            pltpu.SemaphoreType.DMA((3,)),
        ],
        compiler_params=pltpu.CompilerParams(
            collective_id=0, has_side_effects=True, vmem_limit_bytes=56 * 1024 * 1024
        ),
        name="both_halves",
    )(
        outgoing,
        lat_own,
        query_big,
        key_up,
        value_up,
        out_proj,
        w_gate[0],
        w_up[0],
        w_down[0],
        target.reshape(row_count, top_count),
        shares,
    )
    return (mixed, moe_out)


def fits_kernel(mesh, *arrays):
    n_ep, n_tp = mesh.shape["ep"], mesh.shape["tp"]
    tokens, routes, latent = arrays[7], arrays[9], arrays[1]
    capacity = 2 * routes.shape[1] * tokens.shape[0] // (n_ep * n_tp) // n_ep
    own_rows = latent.shape[0] // (n_ep * n_tp)
    packed = latent.shape[0] <= 2048
    return n_tp == 4 and n_ep >= 8 and n_ep % 2 == 0 and capacity % 16 == 0 and own_rows % 16 == 0 and packed


def mapped(mesh, chosen):
    return jax.shard_map(
        chosen,
        mesh=mesh,
        in_specs=(
            P("ep", "tp"),
            P(("ep", "tp"), None),
            P(("ep", "tp"), None),
            P(),
            P(None, "tp"),
            P(None, "tp"),
            P(),
            P(("ep", "tp"), None),
            P(),
            P(("ep", "tp"), None),
            P(("ep", "tp")),
            P(("ep", "tp"), None),
            P("ep", None, "tp"),
            P("ep", None, "tp"),
            P("ep", "tp", None),
        ),
        out_specs=(P(("ep", "tp"), None), P(("ep", "tp"), None)),
        check_vma=False,
    )


def solution(mesh):
    def whole(*arrays):
        chosen = fused_body if fits_kernel(mesh, *arrays) else body
        return mapped(mesh, chosen)(*arrays)

    return whole
```
